32 devices in a mesh: sp: 16 (over z, y, x), tp: 2 (over core).
Axes of the slice: x: 2, y: 2, z: 4, core: 2. Of those that a mesh axis runs over, the one named last changes fastest.
Arguments:
- skip_pathway: bfloat16 [2048, 2048], P('sp', 'tp'), may hold values from -6 to 6
- request_vectors: bfloat16 [2048, 1024], P('sp', 'tp'), may hold values from -6 to 6
- lookup_address_matrix: bfloat16 [2048, 1024], P('sp', 'tp'), may hold values from -6 to 6
- content_vectors: bfloat16 [2048, 1024], P('sp', 'tp'), may hold values from -6 to 6
- result_valve_matrix: bfloat16 [2048, 1024], P('sp', 'tp'), may hold values from -6 to 6
- shrink_raw_signal: float32 [2, 8, 2048], P(None, 'tp', 'sp'), may hold values from -3.1 to 3.6
- channel_shrink_speed: float32 [2, 8], P(None, 'tp'), may hold values from 2.4414063e-05 to 0.05
- insertion_raw_signal: float32 [2, 8, 2048], P(None, 'tp', 'sp'), may hold values from -8.5 to 2
- extra_shrink_spike: float32 [2, 8, 2048], P(None, 'tp', 'sp'), may hold values from -1.2 to 0
- channel_scaling_vector: float32 [128], replicated, may hold values from 0.1 to 1.9
- final_mapping_matrix: bfloat16 [1024, 2048], P(None, 'tp'), may hold values from -0.1875 to 0.1875
- mixer_scaling_vector: float32 [2048], replicated, may hold values from 0.1 to 1.9
- valve_matrix: bfloat16 [2048, 5120], P('sp', 'tp'), may hold values from -0.125 to 0.125
- widening_matrix: bfloat16 [2048, 5120], P('sp', 'tp'), may hold values from -0.125 to 0.125
- temporal_kernel_entries: float32 [3, 5120], P(None, 'tp'), may hold values from -3 to 3
- narrowing_matrix: bfloat16 [5120, 2048], P('tp', 'sp'), may hold values from -0.078125 to 0.078125
Outputs:
- result: bfloat16 [2048, 2048], P('sp', 'tp')
The draws below stay inside these ranges and needn't reach their ends.
All inputs are finite; a program needn't handle non-finite values.
Results may differ from the reference program's by a relative error of at most 0.009.
Values may be sent and summed in bfloat16 or wider, within the bound.
A program may use at most 128 MiB of HBM per device.

```python
import math
import jax
import jax.numpy as jnp
from jax import lax

D = 2048
H = 8
DK = 128
DV = 128
FF = 5120
BLOCK = 64
TOK_DEV = 128
TOKENS = 2048
N_TP = 2


def head_kinds(key):
    share = 0.5
    return jax.random.bernoulli(jax.random.fold_in(key, 11), share, (2, H))


def draw_channel_shrink_speed(key, part):
    slow_head = head_kinds(key)
    slow_rate = jnp.exp(jax.random.uniform(jax.random.fold_in(key, 12), (2, H), jnp.float32, math.log(0.05), math.log(0.5))) / TOKENS
    fast_rate = jnp.exp(jax.random.uniform(jax.random.fold_in(key, 13), (2, H), jnp.float32, math.log(0.015), math.log(0.05)))
    return jnp.where(slow_head, slow_rate, fast_rate).astype(jnp.float32)


def draw_insertion_raw_signal(key, part):
    slow_head = head_kinds(key)
    base = jax.random.truncated_normal(jax.random.fold_in(key, 14), -2.0, 2.0, (2, H, TOKENS), jnp.float32)
    return jnp.where(slow_head[:, :, None], base - 6.5, base).astype(jnp.float32)


def draw_shrink_raw_signal(key, part):
    base = 0.7 * jax.random.truncated_normal(jax.random.fold_in(key, 15), -3.0, 3.0, (2, H, TOKENS), jnp.float32)
    offsets = jax.random.uniform(jax.random.fold_in(key, 16), (2, 1, TOKENS // TOK_DEV), jnp.float32, -1.0, 1.5)
    return (base + jnp.repeat(offsets, TOK_DEV, axis=2)).astype(jnp.float32)


def draw_extra_shrink_spike(key, part):
    places = jax.random.randint(jax.random.fold_in(key, 17), (2, H, 2), 0, TOKENS)
    amounts = jnp.log(jax.random.uniform(jax.random.fold_in(key, 18), (2, H, 2), jnp.float32, 0.55, 0.8))
    positions = jnp.arange(TOKENS, dtype=jnp.int32)
    hits = positions[None, None, None, :] == places[..., None]
    return jnp.sum(jnp.where(hits, amounts[..., None], 0.0), axis=2).astype(jnp.float32)


def shard_levels(stream_key, extent, pieces, low, high):
    level, own = 1.0, jax.random.fold_in(stream_key, 6)
    for axis_at, blocks in pieces:
        steps = jnp.exp(jax.random.uniform(jax.random.fold_in(own, axis_at), (blocks,), jnp.float32, low / len(pieces), high / len(pieces)))
        level = level * jnp.repeat(steps, extent[axis_at] // blocks).reshape([-1 if axis == axis_at else 1 for axis in range(len(extent))])
    return level


def scatter_about(stream_key, dims, scale, reach, cuts=(), kind=jnp.bfloat16):
    loudness = shard_levels(stream_key, dims, cuts, -0.22, 0.18) if cuts else 1.0
    entries = jax.random.normal(stream_key, dims, jnp.float32) * scale * loudness
    return jnp.minimum(jnp.maximum(entries, -reach), reach).astype(kind)


def setup_inputs(seed: int = 0) -> dict:
    arg_keys = jax.random.split(jax.random.key(seed), 17)
    return {
        "skip_pathway": scatter_about(arg_keys[0], (TOKENS, D), 1.0, 6.0, ((0, 16), (1, 2))),
        "request_vectors": scatter_about(arg_keys[1], (TOKENS, H * DK), 1.0, 6.0, ((0, 16), (1, 2))),
        "lookup_address_matrix": scatter_about(arg_keys[2], (TOKENS, H * DK), 1.0, 6.0, ((0, 16), (1, 2))),
        "content_vectors": scatter_about(arg_keys[3], (TOKENS, H * DV), 1.0, 6.0, ((0, 16), (1, 2))),
        "result_valve_matrix": scatter_about(arg_keys[4], (TOKENS, H * DV), 1.5, 6.0, ((0, 16), (1, 2))),
        "shrink_raw_signal": draw_shrink_raw_signal(jax.random.fold_in(arg_keys[16], 71), 0),
        "channel_shrink_speed": draw_channel_shrink_speed(jax.random.fold_in(arg_keys[16], 71), 0),
        "insertion_raw_signal": draw_insertion_raw_signal(jax.random.fold_in(arg_keys[16], 71), 0),
        "extra_shrink_spike": draw_extra_shrink_spike(jax.random.fold_in(arg_keys[16], 71), 0),
        "channel_scaling_vector": jnp.clip(1.0 + 0.18 * jax.random.normal(arg_keys[9], (DV,), jnp.float32), 0.1, 1.9),
        "final_mapping_matrix": scatter_about(arg_keys[10], (H * DV, D), (H * DV) ** -0.5, 0.1875, ((1, 2),)),
        "mixer_scaling_vector": jnp.clip(1.0 + 0.18 * jax.random.normal(arg_keys[11], (D,), jnp.float32), 0.1, 1.9),
        "valve_matrix": scatter_about(arg_keys[12], (D, FF), D ** -0.5, 0.125, ((0, 16), (1, 2))),
        "widening_matrix": scatter_about(arg_keys[13], (D, FF), D ** -0.5, 0.125, ((0, 16), (1, 2))),
        "temporal_kernel_entries": scatter_about(arg_keys[14], (3, FF), 0.5, 3.0, ((1, 2),), jnp.float32),
        "narrowing_matrix": scatter_about(arg_keys[15], (FF, D), FF ** -0.5, 0.078125, ((0, 2), (1, 16))),
    }


HIGHEST = lax.Precision.HIGHEST

def heads_of(matrix, head_size):
    return jnp.transpose(matrix.astype(jnp.float32).reshape(matrix.shape[0], -1, head_size), (1, 0, 2))

def unit_rows(vectors):
    return vectors * lax.rsqrt(lax.optimization_barrier(jnp.sum(vectors * vectors, axis=-1, keepdims=True)) + 1e-06)

def inverse_unit_lower(strict):
    width = strict.shape[-1]
    identity = jnp.eye(width, dtype=jnp.float32)
    powered = -strict
    result = identity + powered
    covered = 2
    while covered < width:
        powered = jnp.matmul(powered, powered, precision=HIGHEST)
        result = jnp.matmul(result, identity + powered, precision=HIGHEST)
        covered = covered * 2
    return result

def block_parts(queries, keys, values, shrink_exponent, beta, width):
    heads, length, key_size = queries.shape
    value_size = values.shape[-1]
    count = length // width
    queries = queries.reshape(heads, count, width, key_size)
    keys = keys.reshape(heads, count, width, key_size)
    values = values.reshape(heads, count, width, value_size)
    shrink_exponent = shrink_exponent.reshape(heads, count, width)
    beta = beta.reshape(heads, count, width)
    cumulative = jnp.cumsum(shrink_exponent, axis=-1)
    inside = jnp.tril(jnp.ones((width, width), dtype=bool))
    decay = jnp.exp(jnp.where(inside, cumulative[..., :, None] - cumulative[..., None, :], -jnp.inf))
    weighted = keys * beta[..., None]
    strict = jnp.tril(jnp.einsum('hnid,hnjd->hnij', weighted, keys, precision=HIGHEST) * decay, -1)
    inverse = inverse_unit_lower(strict)
    writes = jnp.matmul(inverse, values * beta[..., None], precision=HIGHEST)
    erases = jnp.matmul(inverse, weighted * jnp.exp(cumulative)[..., None], precision=HIGHEST)
    within = jnp.einsum('hnid,hnjd->hnij', queries, keys, precision=HIGHEST) * decay
    query_decayed = queries * jnp.exp(cumulative)[..., None]
    keys_decayed = keys * jnp.exp(cumulative[..., -1:] - cumulative)[..., None]
    block_decay = jnp.exp(cumulative[..., -1])
    return (query_decayed, keys_decayed, erases, writes, within, block_decay)

def run_blocks(parts, state):

    def advance(carry, block):
        query_decayed, keys_decayed, erases, writes, within, block_decay = block
        fresh = writes - jnp.matmul(erases, carry, precision=HIGHEST)
        output = jnp.matmul(query_decayed, carry, precision=HIGHEST) + jnp.matmul(within, fresh, precision=HIGHEST)
        carry = carry * block_decay[:, None, None] + jnp.matmul(jnp.swapaxes(keys_decayed, -1, -2), fresh, precision=HIGHEST)
        return (carry, output)
    blocks = tuple((jnp.moveaxis(item, 1, 0) for item in parts))
    final, outputs = lax.scan(advance, state, blocks)
    outputs = jnp.moveaxis(outputs, 0, 1)
    return outputs.reshape(outputs.shape[0], -1, outputs.shape[-1])

def gate_heads(mixture, result_valve_matrix, channel_scaling_vector):
    scaled = mixture * lax.rsqrt(lax.optimization_barrier(jnp.mean(mixture * mixture, axis=-1, keepdims=True)) + 1e-06) * channel_scaling_vector
    gated = scaled * jax.nn.silu(heads_of(result_valve_matrix, mixture.shape[-1]))
    return jnp.transpose(gated, (1, 0, 2)).reshape(gated.shape[1], -1).astype(jnp.bfloat16)

def rms_rows(rows, gain):
    widened = rows.astype(jnp.float32)
    return (widened * lax.rsqrt(lax.optimization_barrier(jnp.mean(widened * widened, axis=-1, keepdims=True)) + 1e-06) * gain).astype(jnp.bfloat16)

def reference(skip_pathway, request_vectors, lookup_address_matrix, content_vectors, result_valve_matrix, shrink_raw_signal, channel_shrink_speed, insertion_raw_signal, extra_shrink_spike, channel_scaling_vector, final_mapping_matrix, mixer_scaling_vector, valve_matrix, widening_matrix, temporal_kernel_entries, narrowing_matrix):
    queries = unit_rows(heads_of(request_vectors, DK)) * DK ** (-0.5)
    keys = unit_rows(heads_of(lookup_address_matrix, DK))
    values = heads_of(content_vectors, DV)
    shrink_exponent = -channel_shrink_speed[:, :, None] * jax.nn.softplus(shrink_raw_signal) + extra_shrink_spike
    beta = jax.nn.sigmoid(insertion_raw_signal)
    empty = jnp.zeros((H, DK, DV), jnp.float32)
    forward = run_blocks(block_parts(queries, keys, values, shrink_exponent[0], beta[0], BLOCK), empty)
    flipped = block_parts(jnp.flip(queries, 1), jnp.flip(keys, 1), jnp.flip(values, 1), jnp.flip(shrink_exponent[1], 1), jnp.flip(beta[1], 1), BLOCK)
    backward = jnp.flip(run_blocks(flipped, empty), 1)
    mixed = gate_heads(forward + backward, result_valve_matrix, channel_scaling_vector)
    projected = jnp.dot(mixed, final_mapping_matrix, preferred_element_type=jnp.float32)
    middle = (skip_pathway.astype(jnp.float32) + projected).astype(jnp.bfloat16)
    normed = rms_rows(middle, mixer_scaling_vector)
    gate = jnp.dot(normed, valve_matrix, preferred_element_type=jnp.float32).astype(jnp.bfloat16)
    up = jnp.dot(normed, widening_matrix, preferred_element_type=jnp.float32)
    padded = jnp.pad(gate, ((1, 1), (0, 0))).astype(jnp.float32)
    convolved = padded[:-2] * temporal_kernel_entries[0] + padded[1:-1] * temporal_kernel_entries[1] + padded[2:] * temporal_kernel_entries[2]
    hidden = (jax.nn.silu(convolved) * up).astype(jnp.bfloat16)
    group = FF // N_TP
    down = jnp.zeros((TOKENS, D), jnp.float32)
    for index in range(N_TP):
        partial_value = jnp.dot(hidden[:, index * group:(index + 1) * group], narrowing_matrix[index * group:(index + 1) * group], preferred_element_type=jnp.float32).astype(jnp.bfloat16)
        partial_value = lax.optimization_barrier(partial_value)
        down = down + partial_value.astype(jnp.float32)
    return (middle.astype(jnp.float32) + down).astype(jnp.bfloat16)
```

```python
import functools

import jax
import jax.numpy as jnp
from jax import lax
from jax.experimental import pallas as pl
from jax.experimental.pallas import tpu as pltpu
from jax.sharding import PartitionSpec as P

DK = 128
DV = 128

HIGH = lax.Precision.HIGH


def heads_of(matrix, head_size):
    return jnp.transpose(
        matrix.astype(jnp.float32).reshape(matrix.shape[0], -1, head_size), (1, 0, 2)
    )


def unit_rows(vectors):
    return vectors * lax.rsqrt(jnp.sum(vectors * vectors, axis=-1, keepdims=True) + 1e-06)


def inverse_unit_triangular(strict):
    width = strict.shape[-1]
    identity = jnp.eye(width, dtype=jnp.float32)
    powered = -strict
    result = identity + powered
    covered = 2
    while covered < width:
        powered = jnp.matmul(powered, powered, precision=HIGH)
        result = result + jnp.matmul(result, powered, precision=HIGH)
        covered = covered * 2
    return result


def local_parts(queries, keys, values, shrink_exponent, beta):
    length = queries.shape[1]
    row = lax.broadcasted_iota(jnp.int32, (length, length), 0)
    column = lax.broadcasted_iota(jnp.int32, (length, length), 1)
    inside = jnp.stack([column <= row, column >= row])[:, None]
    proper = jnp.stack([column < row, column > row])[:, None]
    cumulative = jnp.sum(jnp.where(inside, shrink_exponent[:, :, None, :], 0.0), axis=-1)
    total = jnp.sum(shrink_exponent, axis=-1, keepdims=True)
    decay = jnp.exp(
        jnp.where(inside, cumulative[..., :, None] - cumulative[..., None, :], -jnp.inf)
    )
    likeness = jnp.einsum("hid,hjd->hij", keys, keys, precision=HIGH)
    asked = jnp.einsum("hid,hjd->hij", queries, keys, precision=HIGH)
    strict = jnp.where(proper, likeness * decay * beta[..., None], 0.0)
    inverse = inverse_unit_triangular(strict)
    lift = jnp.exp(cumulative)[..., None]
    right = jnp.concatenate(
        [values * beta[..., None], keys * (beta[..., None] * lift)], axis=-1
    )
    solved = jnp.matmul(inverse, right, precision=HIGH)
    within = asked * decay
    keys_decayed = keys * jnp.exp(total - cumulative)[..., None]
    seen = jnp.matmul(within, solved, precision=HIGH)
    kept = jnp.einsum("ghti,ghtj->ghji", keys_decayed, solved, precision=HIGH)
    dv = values.shape[-1]
    start = jnp.sum(seen[..., :dv], axis=0)
    reach = queries * lift - seen[..., dv:]
    return start, reach, kept, total


def relay_kernel(n, per_direction, dk, maps_ref, out_ref):
    backward = lax.axis_index("sp") >= per_direction
    state = jnp.zeros(out_ref.shape[1:], jnp.float32)
    for step in range(n):
        at = jnp.where(backward, n - 1 - step, step)
        out_ref[at] = state.astype(out_ref.dtype)
        if step < n - 1:
            change = maps_ref[at, :dk, :]
            added = maps_ref[at, dk:, :].astype(jnp.float32)
            upper = state.astype(jnp.bfloat16)
            lower = (state - upper.astype(jnp.float32)).astype(jnp.bfloat16)
            moved = jnp.dot(upper, change, preferred_element_type=jnp.float32)
            moved = moved + jnp.dot(lower, change, preferred_element_type=jnp.float32)
            state = state + moved + added


def entering_states(change, added):
    n = lax.axis_size("sp")
    heads, dk = change.shape[1], change.shape[-1]
    dv = added.shape[2]
    share = n // (2 * heads)
    piece = dv // share
    maps = jnp.concatenate(
        [
            jnp.broadcast_to(change[:, :, None], (2, heads, share, dk, dk)),
            added.reshape(2, heads, share, piece, dk),
        ],
        axis=3,
    ).astype(jnp.bfloat16)
    maps = lax.all_to_all(maps.reshape(n, dk + piece, dk), "sp", 0, 0, tiled=True)
    states = pl.pallas_call(
        functools.partial(relay_kernel, n, n // 2, dk),
        out_shape=jax.ShapeDtypeStruct((n, piece, dk), jnp.bfloat16),
        in_specs=[pl.BlockSpec(memory_space=pltpu.VMEM)],
        out_specs=pl.BlockSpec(memory_space=pltpu.VMEM),
    )(maps)
    states = lax.all_to_all(states, "sp", 0, 0, tiled=True)
    return states.reshape(2, heads, dv, dk)


def gate_heads(mixture, result_valve_matrix, channel_scaling_vector):
    scaled = (
        mixture
        * lax.rsqrt(jnp.mean(mixture * mixture, axis=-1, keepdims=True) + 1e-06)
        * channel_scaling_vector
    )
    gated = scaled * jax.nn.silu(heads_of(result_valve_matrix, mixture.shape[-1]))
    return jnp.transpose(gated, (1, 0, 2)).reshape(gated.shape[1], -1).astype(jnp.bfloat16)


def rms_rows(rows, gain):
    widened = rows.astype(jnp.float32)
    return (
        widened * lax.rsqrt(jnp.mean(widened * widened, axis=-1, keepdims=True) + 1e-06) * gain
    ).astype(jnp.bfloat16)


def group_size(n):
    size = 1
    while 4 * size * size <= n:
        size = size * 2
    return size


def trade(pieces_for, stride, count):
    n = lax.axis_size("sp")
    place = lax.rem(lax.axis_index("sp") // stride, count)
    own = pieces_for(place)
    gathered = lax.dynamic_update_index_in_dim(
        jnp.zeros((count,) + own.shape, own.dtype), own, place, 0
    )
    for flip in range(1, count):
        other = lax.bitwise_xor(place, flip)
        route = [(s, s + ((((s // stride) % count) ^ flip) - (s // stride) % count) * stride) for s in range(n)]
        arrived = lax.ppermute(pieces_for(other), "sp", route)
        gathered = lax.dynamic_update_index_in_dim(gathered, arrived, other, 0)
    return gathered


def swap_within(array, dim, group):
    width = array.shape[dim] // group
    return trade(
        lambda member: lax.dynamic_slice_in_dim(array, member * width, width, axis=dim),
        1,
        group,
    )


def plain_body(
    skip_pathway,
    request_vectors,
    lookup_address_matrix,
    content_vectors,
    result_valve_matrix,
    shrink_raw_signal,
    channel_shrink_speed,
    insertion_raw_signal,
    extra_shrink_spike,
    channel_scaling_vector,
    final_mapping_matrix,
    mixer_scaling_vector,
    valve_matrix,
    widening_matrix,
    temporal_kernel_entries,
    narrowing_matrix,
):
    n = lax.axis_size("sp")
    group = group_size(n)
    place = lax.rem(lax.axis_index("sp"), group)
    far = [[o * group + i for o in range(n // group)] for i in range(group)]

    def collect(pieces):
        return lax.all_gather(pieces, "sp", axis=0, tiled=True, axis_index_groups=far)

    valve = swap_within(valve_matrix, 1, group)
    widening = swap_within(widening_matrix, 1, group)
    valve, widening, request_vectors, lookup_address_matrix = lax.optimization_barrier(
        (valve, widening, request_vectors, lookup_address_matrix)
    )
    valve = collect(valve)
    valve = valve.reshape(-1, valve.shape[-1])
    widening = collect(widening)
    widening = widening.reshape(-1, widening.shape[-1])
    narrowing = collect(swap_within(narrowing_matrix, 0, group))
    units = valve.shape[-1]
    taps = lax.dynamic_slice_in_dim(temporal_kernel_entries, place * units, units, axis=1)

    queries = unit_rows(heads_of(request_vectors, DK)) * DK ** (-0.5)
    keys = unit_rows(heads_of(lookup_address_matrix, DK))
    values = heads_of(content_vectors, DV)
    shrink_exponent = (
        -channel_shrink_speed[:, :, None] * jax.nn.softplus(shrink_raw_signal) + extra_shrink_spike
    )
    beta = jax.nn.sigmoid(insertion_raw_signal)
    start, reach, kept, total = local_parts(queries, keys, values, shrink_exponent, beta)
    added = kept[:, :, :DV]
    change = (
        jnp.expm1(total)[..., None] * jnp.eye(DK, dtype=jnp.float32) - kept[:, :, DV:]
    )
    states = entering_states(change, added)
    carried = jnp.einsum(
        "ghtk,ghvk->ghtv",
        reach.astype(jnp.bfloat16),
        states,
        preferred_element_type=jnp.float32,
    )
    mixture = start + carried[0] + carried[1]
    mixed = gate_heads(mixture, result_valve_matrix, channel_scaling_vector)
    projected = jnp.dot(
        lax.all_gather(mixed, "tp", axis=1, tiled=True),
        final_mapping_matrix,
        preferred_element_type=jnp.float32,
    )
    middle = (skip_pathway.astype(jnp.float32) + projected).astype(jnp.bfloat16)
    rows = trade(lambda member: middle, 1, group)
    full_rows = jnp.concatenate(
        [lax.all_gather(rows[i], "tp", axis=1, tiled=True) for i in range(group)], axis=0
    )
    normed = rms_rows(full_rows, mixer_scaling_vector)

    gate = jnp.dot(normed, valve, preferred_element_type=jnp.float32).astype(jnp.bfloat16)
    before = lax.ppermute(gate[-1:], "sp", [(s, s + group) for s in range(n - group)])
    after = lax.ppermute(gate[:1], "sp", [(s + group, s) for s in range(n - group)])
    up = jnp.dot(normed, widening, preferred_element_type=jnp.float32)
    padded = jnp.concatenate([before, gate, after], axis=0).astype(jnp.float32)
    convolved = padded[:-2] * taps[0] + padded[1:-1] * taps[1] + padded[2:] * taps[2]
    hidden = (jax.nn.silu(convolved) * up).astype(jnp.bfloat16)
    terms = jnp.einsum(
        "th,nhf->tnf", hidden, narrowing, preferred_element_type=jnp.float32
    ).reshape(hidden.shape[0], -1)
    summed = lax.psum_scatter(
        terms.astype(jnp.bfloat16), "tp", scatter_dimension=1, tiled=True
    )
    summed_parts = summed.reshape((group, -1) + summed.shape[1:])
    summed = trade(
        lambda member: lax.dynamic_index_in_dim(summed_parts, member, 0, keepdims=False),
        1,
        group,
    )
    summed = jnp.sum(summed.astype(jnp.float32), axis=0)
    return (middle.astype(jnp.float32) + summed).astype(jnp.bfloat16)


BF = jnp.bfloat16
F32 = jnp.float32
MESH = pl.DeviceIdType.MESH
EPS = 1e-06


def dot(a, b):
    return jnp.dot(a, b, preferred_element_type=F32)


def dot_last(a, b):
    return lax.dot_general(a, b, (((1,), (1,)), ((), ())), preferred_element_type=F32)


def dot_first(a, b):
    return lax.dot_general(a, b, (((0,), (0,)), ((), ())), preferred_element_type=F32)


def flipped(index, mask):
    result = index
    bit = 1
    while bit <= mask:
        if mask & bit:
            result = result + (1 - 2 * ((index // bit) % 2)) * bit
        bit = bit * 2
    return result


def carry_on(state, change):
    upper = state.astype(BF)
    lower = (state - upper.astype(F32)).astype(BF)
    return state + dot(upper, change) + dot(lower, change)


def silu(x):
    return x / (1.0 + jnp.exp(-x))


class Flights:
    def __init__(self):
        self.sent = []

    def send(self, src, dst, send_sem, recv_sem, device):
        copy = pltpu.make_async_remote_copy(
            src_ref=src, dst_ref=dst, send_sem=send_sem, recv_sem=recv_sem,
            device_id=device, device_id_type=MESH,
        )
        copy.start()
        self.sent.append(copy)

    def finish(self):
        for copy in self.sent:
            copy.wait_send()


def landed(dst, send_sem, recv_sem, device):
    pltpu.make_async_remote_copy(
        src_ref=dst, dst_ref=dst, send_sem=send_sem, recv_sem=recv_sem,
        device_id=device, device_id_type=MESH,
    ).wait_recv()


def layer_kernel(
    n, group,
    skip_ref, q_ref, k_ref, v_ref, z_ref, shrink_ref, speed_ref, insert_ref, spike_ref,
    head_gain_ref, fm_ref, row_gain_ref, valve_ref, widening_ref, taps_ref, narrowing_ref,
    out_ref,
    fm, wv, wu, wn, maps_out, maps_in, tot_out, tot_in, st_out, st_in, reach, start, mixbuf,
    tok, nrm, edge_out, edge_in, halo, x_out, x_in, mine, z_out, z_in,
    local_sem, wz_send, wz_recv, wp_send, wp_recv, map_send, map_recv, tot_send, tot_recv,
    st_send, st_recv, mix_send, mix_recv, edge_send, edge_recv, tok_send, tok_recv,
    halo_send, halo_recv, half_send, half_recv, hh_send, hh_recv, x_send, x_recv, z_send, z_recv,
):
    G, F = group, n // group
    nb = F.bit_length() - 1
    length, feats = skip_ref.shape
    heads = q_ref.shape[1] // DK
    units = wv.shape[2]
    cols = narrowing_ref.shape[1]
    s, t = lax.axis_index("sp"), lax.axis_index("tp")
    o, i = s // F, s % F
    other = 1 - t
    after, before = (s + 1) % n, (s + n - 1) % n
    flights = Flights()

    def level(r):
        return (o + r) % G

    barrier = pltpu.get_barrier_semaphore()
    peers = [(s, other), (after, t), (before, t)]
    peers += [(level(r) * F + i, t) for r in range(1, G)]
    peers += [(o * F + (i + r) % F, t) for r in range(1, F)]
    for peer in peers:
        pl.semaphore_signal(barrier, inc=1, device_id=peer, device_id_type=MESH)

    sources = (valve_ref, widening_ref, narrowing_ref)

    def piece(w, lev):
        if w < 2:
            return sources[w].at[:, pl.ds(pl.multiple_of(lev * units, 128), units)]
        return sources[w].at[pl.ds(pl.multiple_of(lev * units, 128), units), :]

    def place(w, block):
        if w < 2:
            return (wv, wu)[w].at[block]
        return wn.at[:, pl.ds(pl.multiple_of(block * cols, 128), cols)]

    local = [pltpu.make_async_copy(fm_ref, fm, local_sem.at[3])]
    local += [pltpu.make_async_copy(piece(w, o), place(w, s), local_sem.at[w]) for w in range(3)]
    for copy in local:
        copy.start()
    pl.semaphore_wait(barrier, len(peers))

    def swap(w):
        for r in range(1, G):
            lev = level(r)
            at = w * G + r
            flights.send(piece(w, lev), place(w, s), wz_send.at[at], wz_recv.at[at], (lev * F + i, t))

    def wait_swap(w, d):
        at = w * G + (G - d) % G
        landed(place(w, level(d) * F + i), wz_send.at[at], wz_recv.at[at], (s, other))

    def order(w, d):
        return [1 << ((d + w + j) % nb) for j in range(nb)]

    def wait_spread(w, d, mask):
        at = (w * G + d) * F + mask
        landed(place(w, level(d) * F + flipped(i, mask)), wp_send.at[at], wp_recv.at[at], (s, other))

    def spread(w, d, stage):
        bits = order(w, d)
        held = [0]
        for b in bits[:stage]:
            held = held + [m + b for m in held]
        if stage == 0 and d > 0:
            wait_swap(w, d)
        for m in held:
            if stage > 0 and m & bits[stage - 1]:
                wait_spread(w, d, m)
        for m in held:
            if m == 0 and d == 0:
                src = piece(w, o)
            else:
                src = place(w, level(d) * F + flipped(i, m))
            at = (w * G + d) * F + m + bits[stage]
            flights.send(
                src, place(w, level(d) * F + flipped(i, m)),
                wp_send.at[at], wp_recv.at[at], (o * F + flipped(i, bits[stage]), t),
            )

    def wait_weights(w):
        local[1 + w].wait()
        for d in range(G):
            bits = order(w, d)
            for m in range(1, F):
                if m & bits[nb - 1]:
                    wait_spread(w, d, m)

    swap(0)
    for w in range(2):
        spread(w, 0, 0)
    swap(1)
    tot_in[o] = jnp.zeros(tot_in.shape[1:], BF)

    row = lax.broadcasted_iota(jnp.int32, (length, length), 0)
    column = lax.broadcasted_iota(jnp.int32, (length, length), 1)
    identity = jnp.where(row == column, 1.0, 0.0).astype(F32)
    R = 2 * heads
    which = lax.broadcasted_iota(jnp.int32, (R, length), 0)
    lane = lax.broadcasted_iota(jnp.int32, (R, length), 1)
    speed = jnp.zeros((R, length), F32)
    for g in range(2):
        for h in range(heads):
            speed = jnp.where(which == g * heads + h, speed_ref[g, h], speed)

    def both(ref):
        return jnp.concatenate([ref[0], ref[1]], axis=0)

    raw = both(shrink_ref)
    softplus = jnp.maximum(raw, 0.0) + jnp.log(1.0 + jnp.exp(-jnp.abs(raw)))
    total_c = both(spike_ref) - speed * softplus
    step = 1
    while step < length:
        ahead = jnp.where(lane >= step, pltpu.roll(total_c, step, 1), 0.0)
        behind = jnp.where(lane < length - step, pltpu.roll(total_c, length - step, 1), 0.0)
        total_c = total_c + jnp.where(which < heads, ahead, behind)
        step = step * 2
    cum = total_c
    total = jnp.where(which[:, :1] < heads, cum[:, length - 1 :], cum[:, :1])
    beta = 1.0 / (1.0 + jnp.exp(-both(insert_ref)))
    pad = jnp.zeros((length - 2 * R, length), F32)
    turned = jnp.transpose(jnp.concatenate([cum, beta, pad], axis=0))

    inside = (column <= row, column >= row)
    proper = (column < row, column > row)

    def crossing(b, g):
        near = row // (2 * b) == column // (2 * b)
        low = ((row // b) % 2 == 1) & ((column // b) % 2 == 0)
        high = ((row // b) % 2 == 0) & ((column // b) % 2 == 1)
        return near & (low if g == 0 else high)

    batch = min(heads, 2)
    for first in range(0, heads, batch):
        some = range(first, first + batch)
        problems = [(h, g) for h in some for g in range(2)]
        keys, queries, keys_b, like, asked = {}, {}, {}, {}, {}
        for h in some:
            k = k_ref[:, h * DK : (h + 1) * DK].astype(F32)
            q = q_ref[:, h * DK : (h + 1) * DK].astype(F32)
            keys[h] = k * lax.rsqrt(jnp.sum(k * k, axis=-1, keepdims=True) + EPS)
            queries[h] = q * (lax.rsqrt(jnp.sum(q * q, axis=-1, keepdims=True) + EPS) * DK ** (-0.5))
            keys_b[h] = keys[h].astype(BF)
            like[h] = dot_last(keys_b[h], keys_b[h])
            asked[h] = dot_last(queries[h].astype(BF), keys_b[h])
        cum_col, beta_col, decay, strict, inverse = {}, {}, {}, {}, {}
        for p in problems:
            h, g = p
            r = g * heads + h
            cum_col[p] = turned[:, r : r + 1]
            beta_col[p] = turned[:, R + r : R + r + 1]
            gap = jnp.where(inside[g], cum_col[p] - cum[r : r + 1, :], -1e30)
            decay[p] = jnp.exp(gap)
            strict[p] = jnp.where(proper[g], like[h] * decay[p] * beta_col[p], 0.0)
            inverse[p] = identity - jnp.where(crossing(1, g), strict[p], 0.0)
        b = 2
        while b < length:
            half, part = {}, {}
            for p in problems:
                half[p] = inverse[p].astype(BF)
                part[p] = jnp.where(crossing(b, p[1]), strict[p], 0.0).astype(BF)
            for p in problems:
                part[p] = dot(part[p], half[p]).astype(BF)
            for p in problems:
                inverse[p] = inverse[p] - dot(half[p], part[p])
            b = b * 2
        solved = {}
        for p in problems:
            h, g = p
            v = v_ref[:, h * DV : (h + 1) * DV].astype(F32)
            lift = jnp.exp(cum_col[p])
            right = jnp.concatenate(
                [(v * beta_col[p]).astype(BF), (keys[h] * (beta_col[p] * lift)).astype(BF)], axis=-1
            )
            solved[p] = dot(inverse[p].astype(BF), right).astype(BF)
        for p in problems:
            h, g = p
            r = g * heads + h
            lift = jnp.exp(cum_col[p])
            seen = dot((asked[h] * decay[p]).astype(BF), solved[p])
            reach[h, :, g * DK : (g + 1) * DK] = (queries[h] * lift - seen[:, DV:]).astype(BF)
            if g == 0:
                start[h] = seen[:, :DV]
            else:
                start[h] = start[h] + seen[:, :DV]
            fading = keys[h] * jnp.exp(total[r : r + 1, :] - cum_col[p])
            kept = dot_first(solved[p], fading.astype(BF))
            maps_out[h, g, :DK] = (identity * (jnp.exp(total[r : r + 1, :]) - 1.0) - kept[DV:]).astype(BF)
            maps_out[h, g, DK:] = kept[:DV].astype(BF)
        for h in some:

            @pl.when(i != h)
            def _():
                pltpu.make_async_remote_copy(
                    src_ref=maps_out.at[h], dst_ref=maps_in.at[i], send_sem=map_send.at[h],
                    recv_sem=map_recv.at[i], device_id=(o * F + h, t), device_id_type=MESH,
                ).start()

            @pl.when(i == h)
            def _():
                maps_in[h] = maps_out[h]

        if first == 0:
            for w in range(2):
                spread(w, 0, 1)
            spread(2, 0, 0)

    for d in range(1, G):
        spread(0, d, 0)

    for j in range(F):

        @pl.when(i != j)
        def _():
            landed(maps_in.at[j], map_send.at[j], map_recv.at[j], (s, other))

    def turn(g, j):
        return j if g == 0 else F - 1 - j

    whole_maps = []
    for g in range(2):
        whole_maps.append(maps_in[turn(g, 0), g].astype(F32))
    for j in range(1, F):
        for g in range(2):
            at = turn(g, j)
            whole_maps[g] = carry_on(whole_maps[g], maps_in[at, g, :DK]) + maps_in[at, g].astype(F32)
    for g in range(2):
        tot_out[g] = whole_maps[g].astype(BF)
    for r in range(1, G):
        flights.send(
            tot_out.at[(o + r) // G], tot_in.at[o], tot_send.at[r], tot_recv.at[r], (level(r) * F + i, t)
        )
    for d in range(1, G):
        spread(0, d, 1)
    for r in range(1, G):
        landed(tot_in.at[level(G - r)], tot_send.at[r], tot_recv.at[r], (s, other))
    states = [jnp.zeros((DV, DK), F32) for _ in range(2)]
    for j in range(G - 1):
        for g in range(2):
            at = j if g == 0 else G - 1 - j
            counts = (at < o) if g == 0 else (at > o)
            m = jnp.where(counts, tot_in[at].astype(F32), 0.0)
            states[g] = carry_on(states[g], m[:DK].astype(BF)) + m[DK:]
    for j in range(F):
        for g in range(2):
            at = turn(g, j)
            st_out[at, :, g * DK : (g + 1) * DK] = states[g].astype(BF)
            if j < F - 1:
                states[g] = carry_on(states[g], maps_in[at, g, :DK]) + maps_in[at, g, DK:].astype(F32)
    for r in range(1, F):
        to = (i + r) % F
        flights.send(st_out.at[to], st_in.at[i], st_send.at[r], st_recv.at[r], (o * F + to, t))
    st_in[i] = st_out[i]
    swap(2)
    for d in range(1, G):
        spread(1, d, 0)
    for r in range(1, F):
        landed(st_in.at[(i + F - r) % F], st_send.at[r], st_recv.at[r], (s, other))

    for h in range(heads):
        mixture = start[h] + dot_last(reach[h], st_in[h])
        scale = lax.rsqrt(jnp.mean(mixture * mixture, axis=-1, keepdims=True) + EPS)
        valve = z_ref[:, h * DV : (h + 1) * DV].astype(F32)
        gated = mixture * scale * head_gain_ref[...] * silu(valve)
        mixbuf[t, :, h * DV : (h + 1) * DV] = gated.astype(BF)
    flights.send(mixbuf.at[t], mixbuf.at[t], mix_send, mix_recv, (s, other))
    local[0].wait()
    wide = heads * DV
    projected = dot(mixbuf[t], fm[pl.ds(pl.multiple_of(t * wide, 128), wide), :])
    landed(mixbuf.at[other], mix_send, mix_recv, (s, other))
    projected = projected + dot(mixbuf[other], fm[pl.ds(pl.multiple_of(other * wide, 128), wide), :])
    middle = (skip_ref[...].astype(F32) + projected).astype(BF)
    tok[o, t] = middle

    flights.send(tok.at[o, t], tok.at[o, t], half_send.at[0], half_recv.at[0], (s, other))
    strips = feats // 128
    ends = jnp.concatenate([middle[:1], middle[length - 1 :]], axis=0).astype(F32)
    edge_out[...] = jnp.concatenate(
        [ends[e : e + 1, c * 128 : (c + 1) * 128] for e in range(2) for c in range(strips)], axis=0
    ).astype(BF)
    flights.send(edge_out, edge_in.at[0], edge_send.at[0], edge_recv.at[0], (after, t))
    flights.send(edge_out, edge_in.at[1], edge_send.at[1], edge_recv.at[1], (before, t))
    for r in range(1, G):
        flights.send(tok.at[o, t], tok.at[o, t], tok_send.at[r], tok_recv.at[r], (level(r) * F + i, t))
    landed(edge_in.at[0], edge_send.at[0], edge_recv.at[0], (s, other))
    landed(edge_in.at[1], edge_send.at[1], edge_recv.at[1], (s, other))
    halo[o, t] = edge_in[...]
    for r in range(1, G):
        flights.send(edge_in, halo.at[o, t], halo_send.at[r], halo_recv.at[r], (level(r) * F + i, t))
    flights.send(edge_in, halo.at[o, t], hh_send.at[0], hh_recv.at[0], (s, other))

    for d in range(1, G):
        spread(1, d, 1)
    spread(2, 0, 1)
    for d in range(1, G):
        spread(2, d, 0)
    wait_weights(0)
    wait_weights(1)
    for d in range(1, G):
        spread(2, d, 1)

    def normed(rows0, rows1):
        squares = jnp.sum(rows0 * rows0, axis=-1, keepdims=True) + jnp.sum(rows1 * rows1, axis=-1, keepdims=True)
        scale = lax.rsqrt(squares * (1.0 / (2 * feats)) + EPS)
        return (
            (rows0 * scale * row_gain_ref[:, :feats]).astype(BF),
            (rows1 * scale * row_gain_ref[:, feats:]).astype(BF),
        )

    def strip_rows(block, half):
        rows = []
        for side in range(2):
            packed = halo[block, half, side].astype(F32)
            base = (1 - side) * strips
            rows.append(jnp.concatenate([packed[base + c : base + c + 1] for c in range(strips)], axis=1))
        return jnp.concatenate(rows + [jnp.zeros((14, feats), F32)], axis=0)

    my_taps = taps_ref[:, pl.ds(pl.multiple_of(o * units, 128), units)]
    row_u = lax.broadcasted_iota(jnp.int32, (length, units), 0)

    def work(r):
        block = level(G - r)
        landed(tok.at[block, other], half_send.at[r], half_recv.at[r], (s, other))
        landed(halo.at[block, other], hh_send.at[r], hh_recv.at[r], (s, other))
        a, b2 = normed(tok[block, 0].astype(F32), tok[block, 1].astype(F32))
        nrm[:length, :feats] = a
        nrm[:length, feats:] = b2
        a, b2 = normed(strip_rows(block, 0), strip_rows(block, 1))
        nrm[length:, :feats] = a
        nrm[length:, feats:] = b2
        gate = dot(nrm[...], wv[...].reshape(2 * feats, units)).astype(BF).astype(F32)
        up = dot(nrm[:length], wu[...].reshape(2 * feats, units))
        at = block * F + i
        first_row = jnp.where(at > 0, gate[length : length + 1], 0.0)
        last_row = jnp.where(at < n - 1, gate[length + 1 : length + 2], 0.0)
        here = gate[:length]
        earlier = jnp.where(row_u == 0, first_row, pltpu.roll(here, 1, 0))
        later = jnp.where(row_u == length - 1, last_row, pltpu.roll(here, length - 1, 0))
        convolved = earlier * my_taps[0:1] + here * my_taps[1:2] + later * my_taps[2:3]
        hidden = (silu(convolved) * up).astype(BF)
        if r == 0:
            wait_weights(2)
        theirs = dot(hidden, wn[:, pl.ds(pl.multiple_of(other * feats, 128), feats)])
        x_out[r] = theirs.astype(BF)
        flights.send(x_out.at[r], x_in.at[r], x_send.at[r], x_recv.at[r], (s, other))
        mine[r] = dot(hidden, wn[:, pl.ds(pl.multiple_of(t * feats, 128), feats)]).astype(BF)

    def settle(r):
        landed(x_in.at[r], x_send.at[r], x_recv.at[r], (s, other))
        both_groups = mine[r].astype(F32) + x_in[r].astype(F32)
        if r == 0:
            return both_groups
        z_out[r] = both_groups.astype(BF)
        flights.send(z_out.at[r], z_in.at[r], z_send.at[r], z_recv.at[r], (level(G - r) * F + i, t))
        return None

    def relay(r):
        block = level(G - r)
        landed(tok.at[block, t], tok_send.at[r], tok_recv.at[r], (s, other))
        flights.send(tok.at[block, t], tok.at[block, t], half_send.at[r], half_recv.at[r], (s, other))
        landed(halo.at[block, t], halo_send.at[r], halo_recv.at[r], (s, other))
        flights.send(halo.at[block, t], halo.at[block, t], hh_send.at[r], hh_recv.at[r], (s, other))

    own = None
    relay(1)
    for r in range(G):
        work(r)
        if r + 2 < G:
            relay(r + 2)
        if r > 0:
            got = settle(r - 1)
            own = got if r == 1 else own
    settle(G - 1)
    result = tok[o, t].astype(F32) + own
    for r in range(1, G):
        landed(z_in.at[r], z_send.at[r], z_recv.at[r], (s, other))
        result = result + z_in[r].astype(F32)
    out_ref[...] = result.astype(BF)

    flights.finish()
    for h in range(heads):

        @pl.when(i != h)
        def _():
            pltpu.make_async_remote_copy(
                src_ref=maps_out.at[h], dst_ref=maps_in.at[i], send_sem=map_send.at[h],
                recv_sem=map_recv.at[i], device_id=(o * F + h, t), device_id_type=MESH,
            ).wait_send()


def fits(n, tp, length, feats, heads, units, rows, cols):
    group = group_size(n)
    far = n // group
    return (
        tp == 2 and group > 1 and far == heads and far & (far - 1) == 0 and heads % 2 == 0
        and length == DK and DK == DV and feats % 128 == 0
        and units % group == 0 and (units // group) % 128 == 0 and cols % 128 == 0 and rows % 16 == 0
    )


def fused_body(
    skip_pathway, request_vectors, lookup_address_matrix, content_vectors, result_valve_matrix,
    shrink_raw_signal, channel_shrink_speed, insertion_raw_signal, extra_shrink_spike,
    channel_scaling_vector, final_mapping_matrix, mixer_scaling_vector, valve_matrix,
    widening_matrix, temporal_kernel_entries, narrowing_matrix,
):
    n = lax.axis_size("sp")
    G = group_size(n)
    F = n // G
    length, feats = skip_pathway.shape
    heads = request_vectors.shape[1] // DK
    rows = valve_matrix.shape[0]
    units = valve_matrix.shape[1] // G
    strips = feats // 128
    vmem, anywhere = pl.BlockSpec(memory_space=pltpu.VMEM), pl.BlockSpec(memory_space=pl.ANY)
    dma = pltpu.SemaphoreType.DMA
    specs = [vmem] * 6 + [pl.BlockSpec(memory_space=pltpu.SMEM)] + [vmem] * 3
    specs += [anywhere, vmem, anywhere, anywhere, vmem, anywhere]
    return pl.pallas_call(
        functools.partial(layer_kernel, n, G),
        out_shape=jax.ShapeDtypeStruct((length, feats), BF),
        in_specs=specs,
        out_specs=vmem,
        scratch_shapes=[
            pltpu.VMEM(final_mapping_matrix.shape, BF),
            pltpu.VMEM((n, rows, units), BF),
            pltpu.VMEM((n, rows, units), BF),
            pltpu.VMEM((units, 2 * feats), BF),
            pltpu.VMEM((heads, 2, DK + DV, DK), BF),
            pltpu.VMEM((F, 2, DK + DV, DK), BF),
            pltpu.VMEM((2, DK + DV, DK), BF),
            pltpu.VMEM((G, DK + DV, DK), BF),
            pltpu.VMEM((F, DV, 2 * DK), BF),
            pltpu.VMEM((heads, DV, 2 * DK), BF),
            pltpu.VMEM((heads, length, 2 * DK), BF),
            pltpu.VMEM((heads, length, DV), F32),
            pltpu.VMEM((2, length, heads * DV), BF),
            pltpu.VMEM((G, 2, length, feats), BF),
            pltpu.VMEM((length + 16, 2 * feats), BF),
            pltpu.VMEM((2 * strips, 128), BF),
            pltpu.VMEM((2, 2 * strips, 128), BF),
            pltpu.VMEM((G, 2, 2, 2 * strips, 128), BF),
            pltpu.VMEM((G, length, feats), BF),
            pltpu.VMEM((G, length, feats), BF),
            pltpu.VMEM((G, length, feats), BF),
            pltpu.VMEM((G, length, feats), BF),
            pltpu.VMEM((G, length, feats), BF),
            dma((4,)),
            dma((3 * G,)), dma((3 * G,)),
            dma((3 * G * F,)), dma((3 * G * F,)),
            dma((F,)), dma((F,)),
            dma((G,)), dma((G,)),
            dma((F,)), dma((F,)),
            dma, dma,
            dma((2,)), dma((2,)),
            dma((G,)), dma((G,)),
            dma((G,)), dma((G,)),
            dma((G,)), dma((G,)),
            dma((G,)), dma((G,)),
            dma((G,)), dma((G,)),
            dma((G,)), dma((G,)),
        ],
        compiler_params=pltpu.CompilerParams(
            collective_id=0, has_side_effects=True, vmem_limit_bytes=60 * 1024 * 1024
        ),
        name="layer",
    )(
        skip_pathway, request_vectors, lookup_address_matrix, content_vectors, result_valve_matrix,
        shrink_raw_signal, channel_shrink_speed, insertion_raw_signal, extra_shrink_spike,
        channel_scaling_vector.reshape(1, -1), final_mapping_matrix, mixer_scaling_vector.reshape(1, -1),
        valve_matrix, widening_matrix, temporal_kernel_entries, narrowing_matrix,
    )


def body(*arrays):
    skip, queries = arrays[0], arrays[1]
    valve, narrowing = arrays[12], arrays[15]
    n, tp = lax.axis_size("sp"), lax.axis_size("tp")
    if fits(n, tp, *skip.shape, queries.shape[1] // DK, valve.shape[1], valve.shape[0], narrowing.shape[1]):
        return fused_body(*arrays)
    return plain_body(*arrays)


def solution(mesh):
    return jax.shard_map(
        body,
        mesh=mesh,
        in_specs=(
            P("sp", "tp"),
            P("sp", "tp"),
            P("sp", "tp"),
            P("sp", "tp"),
            P("sp", "tp"),
            P(None, "tp", "sp"),
            P(None, "tp"),
            P(None, "tp", "sp"),
            P(None, "tp", "sp"),
            P(),
            P(None, "tp"),
            P(),
            P("sp", "tp"),
            P("sp", "tp"),
            P(None, "tp"),
            P("tp", "sp"),
        ),
        out_specs=P("sp", "tp"),
        check_vma=False,
    )
```

```python
import functools

import jax
import jax.numpy as jnp
from jax import lax
from jax.experimental import pallas as pl
from jax.experimental.pallas import tpu as pltpu
from jax.sharding import PartitionSpec as P

DK = 128
DV = 128

HIGH = lax.Precision.HIGH


def heads_of(matrix, head_size):
    return jnp.transpose(
        matrix.astype(jnp.float32).reshape(matrix.shape[0], -1, head_size), (1, 0, 2)
    )


def unit_rows(vectors):
    return vectors * lax.rsqrt(jnp.sum(vectors * vectors, axis=-1, keepdims=True) + 1e-06)


def inverse_unit_triangular(strict):
    width = strict.shape[-1]
    identity = jnp.eye(width, dtype=jnp.float32)
    powered = -strict
    result = identity + powered
    covered = 2
    while covered < width:
        powered = jnp.matmul(powered, powered, precision=HIGH)
        result = result + jnp.matmul(result, powered, precision=HIGH)
        covered = covered * 2
    return result


def local_parts(queries, keys, values, shrink_exponent, beta):
    length = queries.shape[1]
    row = lax.broadcasted_iota(jnp.int32, (length, length), 0)
    column = lax.broadcasted_iota(jnp.int32, (length, length), 1)
    inside = jnp.stack([column <= row, column >= row])[:, None]
    proper = jnp.stack([column < row, column > row])[:, None]
    cumulative = jnp.sum(jnp.where(inside, shrink_exponent[:, :, None, :], 0.0), axis=-1)
    total = jnp.sum(shrink_exponent, axis=-1, keepdims=True)
    decay = jnp.exp(
        jnp.where(inside, cumulative[..., :, None] - cumulative[..., None, :], -jnp.inf)
    )
    likeness = jnp.einsum("hid,hjd->hij", keys, keys, precision=HIGH)
    asked = jnp.einsum("hid,hjd->hij", queries, keys, precision=HIGH)
    strict = jnp.where(proper, likeness * decay * beta[..., None], 0.0)
    inverse = inverse_unit_triangular(strict)
    lift = jnp.exp(cumulative)[..., None]
    right = jnp.concatenate(
        [values * beta[..., None], keys * (beta[..., None] * lift)], axis=-1
    )
    solved = jnp.matmul(inverse, right, precision=HIGH)
    within = asked * decay
    keys_decayed = keys * jnp.exp(total - cumulative)[..., None]
    seen = jnp.matmul(within, solved, precision=HIGH)
    kept = jnp.einsum("ghti,ghtj->ghji", keys_decayed, solved, precision=HIGH)
    dv = values.shape[-1]
    start = jnp.sum(seen[..., :dv], axis=0)
    reach = queries * lift - seen[..., dv:]
    return start, reach, kept, total


def relay_kernel(n, per_direction, dk, maps_ref, out_ref):
    backward = lax.axis_index("sp") >= per_direction
    state = jnp.zeros(out_ref.shape[1:], jnp.float32)
    for step in range(n):
        at = jnp.where(backward, n - 1 - step, step)
        out_ref[at] = state.astype(out_ref.dtype)
        if step < n - 1:
            change = maps_ref[at, :dk, :]
            added = maps_ref[at, dk:, :].astype(jnp.float32)
            upper = state.astype(jnp.bfloat16)
            lower = (state - upper.astype(jnp.float32)).astype(jnp.bfloat16)
            moved = jnp.dot(upper, change, preferred_element_type=jnp.float32)
            moved = moved + jnp.dot(lower, change, preferred_element_type=jnp.float32)
            state = state + moved + added


def entering_states(change, added):
    n = lax.axis_size("sp")
    heads, dk = change.shape[1], change.shape[-1]
    dv = added.shape[2]
    share = n // (2 * heads)
    piece = dv // share
    maps = jnp.concatenate(
        [
            jnp.broadcast_to(change[:, :, None], (2, heads, share, dk, dk)),
            added.reshape(2, heads, share, piece, dk),
        ],
        axis=3,
    ).astype(jnp.bfloat16)
    maps = lax.all_to_all(maps.reshape(n, dk + piece, dk), "sp", 0, 0, tiled=True)
    states = pl.pallas_call(
        functools.partial(relay_kernel, n, n // 2, dk),
        out_shape=jax.ShapeDtypeStruct((n, piece, dk), jnp.bfloat16),
        in_specs=[pl.BlockSpec(memory_space=pltpu.VMEM)],
        out_specs=pl.BlockSpec(memory_space=pltpu.VMEM),
    )(maps)
    states = lax.all_to_all(states, "sp", 0, 0, tiled=True)
    return states.reshape(2, heads, dv, dk)


def gate_heads(mixture, result_valve_matrix, channel_scaling_vector):
    scaled = (
        mixture
        * lax.rsqrt(jnp.mean(mixture * mixture, axis=-1, keepdims=True) + 1e-06)
        * channel_scaling_vector
    )
    gated = scaled * jax.nn.silu(heads_of(result_valve_matrix, mixture.shape[-1]))
    return jnp.transpose(gated, (1, 0, 2)).reshape(gated.shape[1], -1).astype(jnp.bfloat16)


def rms_rows(rows, gain):
    widened = rows.astype(jnp.float32)
    return (
        widened * lax.rsqrt(jnp.mean(widened * widened, axis=-1, keepdims=True) + 1e-06) * gain
    ).astype(jnp.bfloat16)


def group_size(n):
    size = 1
    while 4 * size * size <= n:
        size = size * 2
    return size


def trade(pieces_for, stride, count):
    n = lax.axis_size("sp")
    place = lax.rem(lax.axis_index("sp") // stride, count)
    own = pieces_for(place)
    gathered = lax.dynamic_update_index_in_dim(
        jnp.zeros((count,) + own.shape, own.dtype), own, place, 0
    )
    for flip in range(1, count):
        other = lax.bitwise_xor(place, flip)
        route = [(s, s + ((((s // stride) % count) ^ flip) - (s // stride) % count) * stride) for s in range(n)]
        arrived = lax.ppermute(pieces_for(other), "sp", route)
        gathered = lax.dynamic_update_index_in_dim(gathered, arrived, other, 0)
    return gathered


def swap_within(array, dim, group):
    width = array.shape[dim] // group
    return trade(
        lambda member: lax.dynamic_slice_in_dim(array, member * width, width, axis=dim),
        1,
        group,
    )


def plain_body(
    skip_pathway,
    request_vectors,
    lookup_address_matrix,
    content_vectors,
    result_valve_matrix,
    shrink_raw_signal,
    channel_shrink_speed,
    insertion_raw_signal,
    extra_shrink_spike,
    channel_scaling_vector,
    final_mapping_matrix,
    mixer_scaling_vector,
    valve_matrix,
    widening_matrix,
    temporal_kernel_entries,
    narrowing_matrix,
):
    n = lax.axis_size("sp")
    group = group_size(n)
    place = lax.rem(lax.axis_index("sp"), group)
    far = [[o * group + i for o in range(n // group)] for i in range(group)]

    def collect(pieces):
        return lax.all_gather(pieces, "sp", axis=0, tiled=True, axis_index_groups=far)

    valve = swap_within(valve_matrix, 1, group)
    widening = swap_within(widening_matrix, 1, group)
    valve, widening, request_vectors, lookup_address_matrix = lax.optimization_barrier(
        (valve, widening, request_vectors, lookup_address_matrix)
    )
    valve = collect(valve)
    valve = valve.reshape(-1, valve.shape[-1])
    widening = collect(widening)
    widening = widening.reshape(-1, widening.shape[-1])
    narrowing = collect(swap_within(narrowing_matrix, 0, group))
    units = valve.shape[-1]
    taps = lax.dynamic_slice_in_dim(temporal_kernel_entries, place * units, units, axis=1)

    queries = unit_rows(heads_of(request_vectors, DK)) * DK ** (-0.5)
    keys = unit_rows(heads_of(lookup_address_matrix, DK))
    values = heads_of(content_vectors, DV)
    shrink_exponent = (
        -channel_shrink_speed[:, :, None] * jax.nn.softplus(shrink_raw_signal) + extra_shrink_spike
    )
    beta = jax.nn.sigmoid(insertion_raw_signal)
    start, reach, kept, total = local_parts(queries, keys, values, shrink_exponent, beta)
    added = kept[:, :, :DV]
    change = (
        jnp.expm1(total)[..., None] * jnp.eye(DK, dtype=jnp.float32) - kept[:, :, DV:]
    )
    states = entering_states(change, added)
    carried = jnp.einsum(
        "ghtk,ghvk->ghtv",
        reach.astype(jnp.bfloat16),
        states,
        preferred_element_type=jnp.float32,
    )
    mixture = start + carried[0] + carried[1]
    mixed = gate_heads(mixture, result_valve_matrix, channel_scaling_vector)
    projected = jnp.dot(
        lax.all_gather(mixed, "tp", axis=1, tiled=True),
        final_mapping_matrix,
        preferred_element_type=jnp.float32,
    )
    middle = (skip_pathway.astype(jnp.float32) + projected).astype(jnp.bfloat16)
    rows = trade(lambda member: middle, 1, group)
    full_rows = jnp.concatenate(
        [lax.all_gather(rows[i], "tp", axis=1, tiled=True) for i in range(group)], axis=0
    )
    normed = rms_rows(full_rows, mixer_scaling_vector)

    gate = jnp.dot(normed, valve, preferred_element_type=jnp.float32).astype(jnp.bfloat16)
    before = lax.ppermute(gate[-1:], "sp", [(s, s + group) for s in range(n - group)])
    after = lax.ppermute(gate[:1], "sp", [(s + group, s) for s in range(n - group)])
    up = jnp.dot(normed, widening, preferred_element_type=jnp.float32)
    padded = jnp.concatenate([before, gate, after], axis=0).astype(jnp.float32)
    convolved = padded[:-2] * taps[0] + padded[1:-1] * taps[1] + padded[2:] * taps[2]
    hidden = (jax.nn.silu(convolved) * up).astype(jnp.bfloat16)
    terms = jnp.einsum(
        "th,nhf->tnf", hidden, narrowing, preferred_element_type=jnp.float32
    ).reshape(hidden.shape[0], -1)
    summed = lax.psum_scatter(
        terms.astype(jnp.bfloat16), "tp", scatter_dimension=1, tiled=True
    )
    summed_parts = summed.reshape((group, -1) + summed.shape[1:])
    summed = trade(
        lambda member: lax.dynamic_index_in_dim(summed_parts, member, 0, keepdims=False),
        1,
        group,
    )
    summed = jnp.sum(summed.astype(jnp.float32), axis=0)
    return (middle.astype(jnp.float32) + summed).astype(jnp.bfloat16)


BF = jnp.bfloat16
F32 = jnp.float32
MESH = pl.DeviceIdType.MESH
EPS = 1e-06


def dot(a, b):
    return jnp.dot(a, b, preferred_element_type=F32)


def dot_last(a, b):
    return lax.dot_general(a, b, (((1,), (1,)), ((), ())), preferred_element_type=F32)


def dot_first(a, b):
    return lax.dot_general(a, b, (((0,), (0,)), ((), ())), preferred_element_type=F32)


def flipped(index, mask):
    result = index
    bit = 1
    while bit <= mask:
        if mask & bit:
            result = result + (1 - 2 * ((index // bit) % 2)) * bit
        bit = bit * 2
    return result


def carry_on(state, change):
    upper = state.astype(BF)
    lower = (state - upper.astype(F32)).astype(BF)
    return state + dot(upper, change) + dot(lower, change)


def silu(x):
    return x / (1.0 + jnp.exp(-x))


def only(when, act):
    if when is True:
        act()
    else:
        pl.when(when)(act)


class Flights:
    def __init__(self):
        self.sent = []

    def send(self, src, dst, send_sem, recv_sem, device, when=True):
        copy = pltpu.make_async_remote_copy(
            src_ref=src, dst_ref=dst, send_sem=send_sem, recv_sem=recv_sem,
            device_id=device, device_id_type=MESH,
        )
        only(when, copy.start)
        self.sent.append((when, copy))

    def finish(self):
        for when, copy in self.sent:
            only(when, copy.wait_send)


class Phases:
    def __init__(self):
        self.scope = None

    def __call__(self, name):
        if self.scope is not None:
            self.scope.__exit__(None, None, None)
        self.scope = jax.named_scope(name) if name else None
        if name:
            self.scope.__enter__()


def landed(dst, send_sem, recv_sem, device):
    pltpu.make_async_remote_copy(
        src_ref=dst, dst_ref=dst, send_sem=send_sem, recv_sem=recv_sem,
        device_id=device, device_id_type=MESH,
    ).wait_recv()


def layer_kernel(
    n, group,
    skip_ref, q_ref, k_ref, v_ref, z_ref, shrink_ref, speed_ref, insert_ref, spike_ref,
    head_gain_ref, fm_ref, row_gain_ref, valve_ref, widening_ref, taps_ref, narrowing_ref,
    out_ref,
    fm, wv, wu, wn, maps_out, maps_in, tot_out, tot_in, st_out, st_in, reach, start, mixbuf,
    tok, nrm, edge_out, edge_in, halo, hid, x_out, x_in, mine, z_out, z_in,
    local_sem, wz_send, wz_recv, wp_send, wp_recv, map_send, map_recv, tot_send, tot_recv,
    st_send, st_recv, mix_send, mix_recv, edge_send, edge_recv, tok_send, tok_recv,
    halo_send, halo_recv, half_send, half_recv, hh_send, hh_recv, x_send, x_recv, z_send, z_recv,
):
    G, F = group, n // group
    nb = F.bit_length() - 1
    length, feats = skip_ref.shape
    heads = q_ref.shape[1] // DK
    units = wv.shape[2]
    cols = narrowing_ref.shape[1]
    s, t = lax.axis_index("sp"), lax.axis_index("tp")
    o, i = s // F, s % F
    other = 1 - t
    after, before = (s + 1) % n, (s + n - 1) % n
    flights = Flights()
    phase = Phases()

    def level(r):
        return (o + r) % G

    barrier = pltpu.get_barrier_semaphore()
    peers = [(s, other), (after, t), (before, t)]
    peers += [(level(r) * F + i, t) for r in range(1, G)]
    peers += [(o * F + (i + r) % F, t) for r in range(1, F)]
    for peer in peers:
        pl.semaphore_signal(barrier, inc=1, device_id=peer, device_id_type=MESH)

    sources = (valve_ref, widening_ref, narrowing_ref)

    def piece(w, lev):
        if w < 2:
            return sources[w].at[:, pl.ds(pl.multiple_of(lev * units, 128), units)]
        return sources[w].at[pl.ds(pl.multiple_of(lev * units, 128), units), :]

    def place(w, block):
        if w < 2:
            return (wv, wu)[w].at[block]
        return wn.at[:, pl.ds(pl.multiple_of(block * cols, 128), cols)]

    local = [pltpu.make_async_copy(fm_ref, fm, local_sem.at[3])]
    local += [pltpu.make_async_copy(piece(w, o), place(w, s), local_sem.at[w]) for w in range(3)]
    for copy in local:
        copy.start()
    phase("barrier")
    pl.semaphore_wait(barrier, len(peers))

    def swap(w):
        for r in range(1, G):
            lev = level(r)
            at = w * G + r
            flights.send(piece(w, lev), place(w, s), wz_send.at[at], wz_recv.at[at], (lev * F + i, t))

    def wait_swap(w, d):
        at = w * G + (G - d) % G
        landed(place(w, level(d) * F + i), wz_send.at[at], wz_recv.at[at], (s, other))

    def order(w, d):
        return [1 << ((d + w + j) % nb) for j in range(nb)]

    def wait_spread(w, d, mask):
        at = (w * G + d) * F + mask
        landed(place(w, level(d) * F + flipped(i, mask)), wp_send.at[at], wp_recv.at[at], (s, other))

    def spread(w, d, stage):
        bits = order(w, d)
        held = [0]
        for b in bits[:stage]:
            held = held + [m + b for m in held]
        if stage == 0 and d > 0:
            wait_swap(w, d)
        for m in held:
            if stage > 0 and m & bits[stage - 1]:
                wait_spread(w, d, m)
        for m in held:
            if m == 0 and d == 0:
                src = piece(w, o)
            else:
                src = place(w, level(d) * F + flipped(i, m))
            at = (w * G + d) * F + m + bits[stage]
            flights.send(
                src, place(w, level(d) * F + flipped(i, m)),
                wp_send.at[at], wp_recv.at[at], (o * F + flipped(i, bits[stage]), t),
            )

    def wait_weights(w):
        local[1 + w].wait()
        for d in range(G):
            bits = order(w, d)
            for m in range(1, F):
                if m & bits[nb - 1]:
                    wait_spread(w, d, m)

    phase("first_sends")
    swap(0)
    for w in range(2):
        spread(w, 0, 0)
    tot_in[o] = jnp.zeros(tot_in.shape[1:], BF)

    phase("setup")
    row = lax.broadcasted_iota(jnp.int32, (length, length), 0)
    column = lax.broadcasted_iota(jnp.int32, (length, length), 1)
    identity = jnp.where(row == column, 1.0, 0.0).astype(F32)
    R = 2 * heads
    which = lax.broadcasted_iota(jnp.int32, (R, length), 0)
    lane = lax.broadcasted_iota(jnp.int32, (R, length), 1)
    speed = jnp.zeros((R, length), F32)
    for g in range(2):
        for h in range(heads):
            speed = jnp.where(which == g * heads + h, speed_ref[g, h], speed)

    def both(ref):
        return jnp.concatenate([ref[0], ref[1]], axis=0)

    raw = both(shrink_ref)
    softplus = jnp.maximum(raw, 0.0) + jnp.log(1.0 + jnp.exp(-jnp.abs(raw)))
    total_c = both(spike_ref) - speed * softplus
    step = 1
    while step < length:
        ahead = jnp.where(lane >= step, pltpu.roll(total_c, step, 1), 0.0)
        behind = jnp.where(lane < length - step, pltpu.roll(total_c, length - step, 1), 0.0)
        total_c = total_c + jnp.where(which < heads, ahead, behind)
        step = step * 2
    cum = total_c
    total = jnp.where(which[:, :1] < heads, cum[:, length - 1 :], cum[:, :1])
    beta = 1.0 / (1.0 + jnp.exp(-both(insert_ref)))
    pad = jnp.zeros((length - 2 * R, length), F32)
    turned = jnp.transpose(jnp.concatenate([cum, beta, pad], axis=0))

    inside = (column <= row, column >= row)
    proper = (column < row, column > row)

    def crossing(b, g):
        near = row // (2 * b) == column // (2 * b)
        low = ((row // b) % 2 == 1) & ((column // b) % 2 == 0)
        high = ((row // b) % 2 == 0) & ((column // b) % 2 == 1)
        return near & (low if g == 0 else high)

    batch = min(heads, 2)
    for first in range(0, heads, batch):
        phase("local_attention")
        some = range(first, first + batch)
        problems = [(h, g) for h in some for g in range(2)]
        keys, queries, keys_b, like, asked = {}, {}, {}, {}, {}
        for h in some:
            k = k_ref[:, h * DK : (h + 1) * DK].astype(F32)
            q = q_ref[:, h * DK : (h + 1) * DK].astype(F32)
            keys[h] = k * lax.rsqrt(jnp.sum(k * k, axis=-1, keepdims=True) + EPS)
            queries[h] = q * (lax.rsqrt(jnp.sum(q * q, axis=-1, keepdims=True) + EPS) * DK ** (-0.5))
            keys_b[h] = keys[h].astype(BF)
            like[h] = dot_last(keys_b[h], keys_b[h])
            asked[h] = dot_last(queries[h].astype(BF), keys_b[h])
        cum_col, beta_col, decay, strict, inverse = {}, {}, {}, {}, {}
        for p in problems:
            h, g = p
            r = g * heads + h
            cum_col[p] = turned[:, r : r + 1]
            beta_col[p] = turned[:, R + r : R + r + 1]
            gap = jnp.where(inside[g], cum_col[p] - cum[r : r + 1, :], -1e30)
            decay[p] = jnp.exp(gap)
            strict[p] = jnp.where(proper[g], like[h] * decay[p] * beta_col[p], 0.0)
            inverse[p] = identity - jnp.where(crossing(1, g), strict[p], 0.0)
        b = 2
        while b < length:
            half, part = {}, {}
            for p in problems:
                half[p] = inverse[p].astype(BF)
                part[p] = jnp.where(crossing(b, p[1]), strict[p], 0.0).astype(BF)
            for p in problems:
                part[p] = dot(part[p], half[p]).astype(BF)
            for p in problems:
                inverse[p] = inverse[p] - dot(half[p], part[p])
            b = b * 2
        solved = {}
        for p in problems:
            h, g = p
            v = v_ref[:, h * DV : (h + 1) * DV].astype(F32)
            lift = jnp.exp(cum_col[p])
            right = jnp.concatenate(
                [(v * beta_col[p]).astype(BF), (keys[h] * (beta_col[p] * lift)).astype(BF)], axis=-1
            )
            solved[p] = dot(inverse[p].astype(BF), right).astype(BF)
        for p in problems:
            h, g = p
            r = g * heads + h
            lift = jnp.exp(cum_col[p])
            seen = dot((asked[h] * decay[p]).astype(BF), solved[p])
            reach[h, :, g * DK : (g + 1) * DK] = (queries[h] * lift - seen[:, DV:]).astype(BF)
            if g == 0:
                start[h] = seen[:, :DV]
            else:
                start[h] = start[h] + seen[:, :DV]
            fading = keys[h] * jnp.exp(total[r : r + 1, :] - cum_col[p])
            kept = dot_first(solved[p], fading.astype(BF))
            maps_out[h, g, :DK] = (identity * (jnp.exp(total[r : r + 1, :]) - 1.0) - kept[DV:]).astype(BF)
            maps_out[h, g, DK:] = kept[:DV].astype(BF)
        phase("send_maps")
        for h in some:
            flights.send(
                maps_out.at[h], maps_in.at[i], map_send.at[h], map_recv.at[i], (o * F + h, t), when=i != h
            )

            @pl.when(i == h)
            def _():
                maps_in[h] = maps_out[h]

    phase("spread_own")
    for w in range(2):
        spread(w, 0, 1)
    spread(2, 0, 0)

    phase("wait_maps")
    for j in range(F):

        @pl.when(i != j)
        def _():
            landed(maps_in.at[j], map_send.at[j], map_recv.at[j], (s, other))

    phase("compose")
    def turn(g, j):
        return j if g == 0 else F - 1 - j

    whole_maps = []
    for g in range(2):
        whole_maps.append(maps_in[turn(g, 0), g].astype(F32))
    for j in range(1, F):
        for g in range(2):
            at = turn(g, j)
            whole_maps[g] = carry_on(whole_maps[g], maps_in[at, g, :DK]) + maps_in[at, g].astype(F32)
    for g in range(2):
        tot_out[g] = whole_maps[g].astype(BF)
    phase("send_totals")
    for r in range(1, G):
        flights.send(
            tot_out.at[(o + r) // G], tot_in.at[o], tot_send.at[r], tot_recv.at[r], (level(r) * F + i, t)
        )
    phase("spread_0_0")
    for d in range(1, G):
        spread(0, d, 0)
    phase("wait_totals")
    for r in range(1, G):
        landed(tot_in.at[level(G - r)], tot_send.at[r], tot_recv.at[r], (s, other))
    swap(1)
    phase("states")
    states = [jnp.zeros((DV, DK), F32) for _ in range(2)]
    for j in range(G - 1):
        for g in range(2):
            at = j if g == 0 else G - 1 - j
            counts = (at < o) if g == 0 else (at > o)
            m = jnp.where(counts, tot_in[at].astype(F32), 0.0)
            states[g] = carry_on(states[g], m[:DK].astype(BF)) + m[DK:]
    for j in range(F):
        for g in range(2):
            at = turn(g, j)
            st_out[at, :, g * DK : (g + 1) * DK] = states[g].astype(BF)
            if j < F - 1:
                states[g] = carry_on(states[g], maps_in[at, g, :DK]) + maps_in[at, g, DK:].astype(F32)
    phase("send_states")
    for r in range(1, F):
        to = (i + r) % F
        flights.send(st_out.at[to], st_in.at[i], st_send.at[r], st_recv.at[r], (o * F + to, t))
    st_in[i] = st_out[i]
    spread(2, 0, 1)
    phase("wait_states")
    for r in range(1, F):
        landed(st_in.at[(i + F - r) % F], st_send.at[r], st_recv.at[r], (s, other))

    phase("outputs")
    for h in range(heads):
        mixture = start[h] + dot_last(reach[h], st_in[h])
        scale = lax.rsqrt(jnp.mean(mixture * mixture, axis=-1, keepdims=True) + EPS)
        valve = z_ref[:, h * DV : (h + 1) * DV].astype(F32)
        gated = mixture * scale * head_gain_ref[...] * silu(valve)
        mixbuf[t, :, h * DV : (h + 1) * DV] = gated.astype(BF)
    flights.send(mixbuf.at[t], mixbuf.at[t], mix_send, mix_recv, (s, other))
    phase("spread_0_1")
    for d in range(1, G):
        spread(0, d, 1)
    phase("project")
    local[0].wait()
    wide = heads * DV
    projected = dot(mixbuf[t], fm[pl.ds(pl.multiple_of(t * wide, 128), wide), :])
    phase("wait_mix")
    landed(mixbuf.at[other], mix_send, mix_recv, (s, other))
    phase("middle")
    projected = projected + dot(mixbuf[other], fm[pl.ds(pl.multiple_of(other * wide, 128), wide), :])
    middle = (skip_ref[...].astype(F32) + projected).astype(BF)
    tok[o, t] = middle

    def share(block, when=True):
        flights.send(
            tok.at[block, t], tok.at[block, t], half_send.at[block], half_recv.at[block], (s, other), when=when
        )

    def pass_up(block, when):
        flights.send(
            tok.at[block, t], tok.at[block, t], tok_send.at[block], tok_recv.at[block],
            (s + F, t), when=when & (o < G - 1),
        )

    def pass_down(block, when):
        flights.send(
            tok.at[block, t], tok.at[block, t], tok_send.at[G + block], tok_recv.at[block],
            (s - F, t), when=when & (o > 0),
        )

    def arrive(distance):
        for below in (True, False):
            block = o - distance if below else o + distance
            there = block >= 0 if below else block < G

            @pl.when(there)
            def _():
                landed(tok.at[block, t], tok_send.at[block], tok_recv.at[block], (s, other))

            share(block, when=there)
            (pass_up if below else pass_down)(block, there)

    pass_up(o, o >= 0)
    pass_down(o, o >= 0)
    share(o)
    strips = feats // 128
    ends = jnp.concatenate([middle[:1], middle[length - 1 :]], axis=0).astype(F32)
    edge_out[...] = jnp.concatenate(
        [ends[e : e + 1, c * 128 : (c + 1) * 128] for e in range(2) for c in range(strips)], axis=0
    ).astype(BF)
    flights.send(edge_out, edge_in.at[0], edge_send.at[0], edge_recv.at[0], (after, t))
    flights.send(edge_out, edge_in.at[1], edge_send.at[1], edge_recv.at[1], (before, t))
    phase("spread_1_0")
    for d in range(1, G):
        spread(1, d, 0)
    phase("rows_1")
    arrive(1)
    phase("spread_1_1")
    for d in range(1, G):
        spread(1, d, 1)
    phase("wait_edges")
    landed(edge_in.at[0], edge_send.at[0], edge_recv.at[0], (s, other))
    landed(edge_in.at[1], edge_send.at[1], edge_recv.at[1], (s, other))
    halo[o, t] = edge_in[...]
    for r in range(1, G):
        flights.send(edge_in, halo.at[o, t], halo_send.at[r], halo_recv.at[r], (level(r) * F + i, t))
    flights.send(edge_in, halo.at[o, t], hh_send.at[0], hh_recv.at[0], (s, other))
    phase("rows_2")
    for distance in range(2, G):
        arrive(distance)
        if distance == max(G - 2, 2):
            swap(2)
    phase("relay_halo")
    for r in range(1, G):
        block = level(G - r)
        landed(halo.at[block, t], halo_send.at[r], halo_recv.at[r], (s, other))
        flights.send(halo.at[block, t], halo.at[block, t], hh_send.at[r], hh_recv.at[r], (s, other))
    phase("wait_weights")
    wait_weights(0)
    wait_weights(1)

    def normed(rows0, rows1):
        squares = jnp.sum(rows0 * rows0, axis=-1, keepdims=True) + jnp.sum(rows1 * rows1, axis=-1, keepdims=True)
        scale = lax.rsqrt(squares * (1.0 / (2 * feats)) + EPS)
        return (
            (rows0 * scale * row_gain_ref[:, :feats]).astype(BF),
            (rows1 * scale * row_gain_ref[:, feats:]).astype(BF),
        )

    def strip_rows(block, half):
        rows = []
        for side in range(2):
            packed = halo[block, half, side].astype(F32)
            base = (1 - side) * strips
            rows.append(jnp.concatenate([packed[base + c : base + c + 1] for c in range(strips)], axis=1))
        return jnp.concatenate(rows + [jnp.zeros((14, feats), F32)], axis=0)

    my_taps = taps_ref[:, pl.ds(pl.multiple_of(o * units, 128), units)]
    row_u = lax.broadcasted_iota(jnp.int32, (length, units), 0)

    def work(r):
        block = level(G - r)
        phase("wait_rows_from_core")
        landed(tok.at[block, other], half_send.at[block], half_recv.at[block], (s, other))
        landed(halo.at[block, other], hh_send.at[r], hh_recv.at[r], (s, other))
        phase("ffn_in")
        a, b2 = normed(tok[block, 0].astype(F32), tok[block, 1].astype(F32))
        nrm[:length, :feats] = a
        nrm[:length, feats:] = b2
        a, b2 = normed(strip_rows(block, 0), strip_rows(block, 1))
        nrm[length:, :feats] = a
        nrm[length:, feats:] = b2
        gate = dot(nrm[...], wv[...].reshape(2 * feats, units)).astype(BF).astype(F32)
        up = dot(nrm[:length], wu[...].reshape(2 * feats, units))
        at = block * F + i
        first_row = jnp.where(at > 0, gate[length : length + 1], 0.0)
        last_row = jnp.where(at < n - 1, gate[length + 1 : length + 2], 0.0)
        here = gate[:length]
        earlier = jnp.where(row_u == 0, first_row, pltpu.roll(here, 1, 0))
        later = jnp.where(row_u == length - 1, last_row, pltpu.roll(here, length - 1, 0))
        convolved = earlier * my_taps[0:1] + here * my_taps[1:2] + later * my_taps[2:3]
        hid[r] = (silu(convolved) * up).astype(BF)

    parts = G // 2
    chunk = F * cols

    def down(d):
        lev = level(d)
        home, q = lev // parts, lev % parts
        product = dot(
            hid[...].reshape(G * length, units), wn[:, pl.ds(pl.multiple_of(lev * chunk, 128), chunk)]
        )

        @pl.when(home != t)
        def _():
            x_out[q] = product.astype(BF).reshape(G, length, chunk)

        flights.send(x_out.at[q], x_in.at[q], x_send.at[q], x_recv.at[q], (s, other), when=home != t)

        @pl.when(home == t)
        def _():
            mine[q] = product.astype(BF).reshape(G, length, chunk)

    def settle(d):
        lev = level(d)
        home, q = lev // parts, lev % parts

        @pl.when(home == t)
        def _():
            landed(x_in.at[q], x_send.at[q], x_recv.at[q], (s, other))
            z_out[q] = (mine[q].astype(F32) + x_in[q].astype(F32)).astype(BF)

        for r in range(1, G):
            flights.send(
                z_out.at[q, r], z_in.at[o, q], z_send.at[q * G + r], z_recv.at[o * parts + q],
                (level(G - r) * F + i, t), when=home == t,
            )

    for r in range(G):
        work(r)
    phase("down_own")
    for m in range(1, F):
        if m & order(2, 0)[nb - 1]:
            wait_spread(2, 0, m)
    local[3].wait()
    down(0)
    phase("spread_2_0")
    for d in range(1, G):
        spread(2, d, 0)
    phase("settle_own")
    settle(0)
    phase("spread_2_1")
    for d in range(1, G):
        spread(2, d, 1)
    for d in range(1, G):
        phase("wait_narrowing")
        for m in range(1, F):
            if m & order(2, d)[nb - 1]:
                wait_spread(2, d, m)
        phase("down")
        down(d)
        phase("settle")
        settle(d)
    phase("result")
    for q in range(parts):
        at = slice(q * chunk, (q + 1) * chunk)
        result = tok[o, t, :, at].astype(F32) + z_out[q, 0].astype(F32)
        for r in range(1, G):
            lev = level(r)
            landed(z_in.at[lev, q], z_send.at[q], z_recv.at[lev * parts + q], (s, other))
            result = result + z_in[lev, q].astype(F32)
        out_ref[:, at] = result.astype(BF)

    phase("finish")
    flights.finish()

    phase(None)


def fits(n, tp, length, feats, heads, units, rows, cols):
    group = group_size(n)
    far = n // group
    return (
        tp == 2 and group > 1 and far == heads and far & (far - 1) == 0 and heads % 2 == 0
        and length == DK and DK == DV and feats % 128 == 0
        and units % group == 0 and (units // group) % 128 == 0 and cols % 128 == 0 and rows % 16 == 0
    )


def fused_body(
    skip_pathway, request_vectors, lookup_address_matrix, content_vectors, result_valve_matrix,
    shrink_raw_signal, channel_shrink_speed, insertion_raw_signal, extra_shrink_spike,
    channel_scaling_vector, final_mapping_matrix, mixer_scaling_vector, valve_matrix,
    widening_matrix, temporal_kernel_entries, narrowing_matrix,
):
    n = lax.axis_size("sp")
    G = group_size(n)
    F = n // G
    length, feats = skip_pathway.shape
    heads = request_vectors.shape[1] // DK
    rows = valve_matrix.shape[0]
    units = valve_matrix.shape[1] // G
    strips = feats // 128
    vmem, anywhere = pl.BlockSpec(memory_space=pltpu.VMEM), pl.BlockSpec(memory_space=pl.ANY)
    dma = pltpu.SemaphoreType.DMA
    specs = [vmem] * 6 + [pl.BlockSpec(memory_space=pltpu.SMEM)] + [vmem] * 3
    specs += [anywhere, vmem, anywhere, anywhere, vmem, anywhere]
    return pl.pallas_call(
        functools.partial(layer_kernel, n, G),
        out_shape=jax.ShapeDtypeStruct((length, feats), BF),
        in_specs=specs,
        out_specs=vmem,
        scratch_shapes=[
            pltpu.VMEM(final_mapping_matrix.shape, BF),
            pltpu.VMEM((n, rows, units), BF),
            pltpu.VMEM((n, rows, units), BF),
            pltpu.VMEM((units, 2 * feats), BF),
            pltpu.VMEM((heads, 2, DK + DV, DK), BF),
            pltpu.VMEM((F, 2, DK + DV, DK), BF),
            pltpu.VMEM((2, DK + DV, DK), BF),
            pltpu.VMEM((G, DK + DV, DK), BF),
            pltpu.VMEM((F, DV, 2 * DK), BF),
            pltpu.VMEM((heads, DV, 2 * DK), BF),
            pltpu.VMEM((heads, length, 2 * DK), BF),
            pltpu.VMEM((heads, length, DV), F32),
            pltpu.VMEM((2, length, heads * DV), BF),
            pltpu.VMEM((G, 2, length, feats), BF),
            pltpu.VMEM((length + 16, 2 * feats), BF),
            pltpu.VMEM((2 * strips, 128), BF),
            pltpu.VMEM((2, 2 * strips, 128), BF),
            pltpu.VMEM((G, 2, 2, 2 * strips, 128), BF),
            pltpu.VMEM((G, length, units), BF),
            pltpu.VMEM((G // 2, G, length, 2 * feats // G), BF),
            pltpu.VMEM((G // 2, G, length, 2 * feats // G), BF),
            pltpu.VMEM((G // 2, G, length, 2 * feats // G), BF),
            pltpu.VMEM((G // 2, G, length, 2 * feats // G), BF),
            pltpu.VMEM((G, G // 2, length, 2 * feats // G), BF),
            dma((4,)),
            dma((3 * G,)), dma((3 * G,)),
            dma((3 * G * F,)), dma((3 * G * F,)),
            dma((F,)), dma((F,)),
            dma((G,)), dma((G,)),
            dma((F,)), dma((F,)),
            dma, dma,
            dma((2,)), dma((2,)),
            dma((2 * G,)), dma((G,)),
            dma((G,)), dma((G,)),
            dma((G,)), dma((G,)),
            dma((G,)), dma((G,)),
            dma((G // 2,)), dma((G // 2,)),
            dma((G * G // 2,)), dma((G * G // 2,)),
        ],
        compiler_params=pltpu.CompilerParams(
            collective_id=0, has_side_effects=True, vmem_limit_bytes=60 * 1024 * 1024
        ),
        name="layer",
    )(
        skip_pathway, request_vectors, lookup_address_matrix, content_vectors, result_valve_matrix,
        shrink_raw_signal, channel_shrink_speed, insertion_raw_signal, extra_shrink_spike,
        channel_scaling_vector.reshape(1, -1), final_mapping_matrix, mixer_scaling_vector.reshape(1, -1),
        valve_matrix, widening_matrix, temporal_kernel_entries, narrowing_matrix,
    )


def body(*arrays):
    skip, queries = arrays[0], arrays[1]
    valve, narrowing = arrays[12], arrays[15]
    n, tp = lax.axis_size("sp"), lax.axis_size("tp")
    if fits(n, tp, *skip.shape, queries.shape[1] // DK, valve.shape[1], valve.shape[0], narrowing.shape[1]):
        return fused_body(*arrays)
    return plain_body(*arrays)


def solution(mesh):
    return jax.shard_map(
        body,
        mesh=mesh,
        in_specs=(
            P("sp", "tp"),
            P("sp", "tp"),
            P("sp", "tp"),
            P("sp", "tp"),
            P("sp", "tp"),
            P(None, "tp", "sp"),
            P(None, "tp"),
            P(None, "tp", "sp"),
            P(None, "tp", "sp"),
            P(),
            P(None, "tp"),
            P(),
            P("sp", "tp"),
            P("sp", "tp"),
            P(None, "tp"),
            P("tp", "sp"),
        ),
        out_specs=P("sp", "tp"),
        check_vma=False,
    )
```

```python
import functools

import jax
import jax.numpy as jnp
from jax import lax
from jax.experimental import pallas as pl
from jax.experimental.pallas import tpu as pltpu
from jax.sharding import PartitionSpec as P

DK = 128
DV = 128

HIGH = lax.Precision.HIGH


def heads_of(matrix, head_size):
    return jnp.transpose(
        matrix.astype(jnp.float32).reshape(matrix.shape[0], -1, head_size), (1, 0, 2)
    )


def unit_rows(vectors):
    return vectors * lax.rsqrt(jnp.sum(vectors * vectors, axis=-1, keepdims=True) + 1e-06)


def inverse_unit_triangular(strict):
    width = strict.shape[-1]
    identity = jnp.eye(width, dtype=jnp.float32)
    powered = -strict
    result = identity + powered
    covered = 2
    while covered < width:
        powered = jnp.matmul(powered, powered, precision=HIGH)
        result = result + jnp.matmul(result, powered, precision=HIGH)
        covered = covered * 2
    return result


def local_parts(queries, keys, values, shrink_exponent, beta):
    length = queries.shape[1]
    row = lax.broadcasted_iota(jnp.int32, (length, length), 0)
    column = lax.broadcasted_iota(jnp.int32, (length, length), 1)
    inside = jnp.stack([column <= row, column >= row])[:, None]
    proper = jnp.stack([column < row, column > row])[:, None]
    cumulative = jnp.sum(jnp.where(inside, shrink_exponent[:, :, None, :], 0.0), axis=-1)
    total = jnp.sum(shrink_exponent, axis=-1, keepdims=True)
    decay = jnp.exp(
        jnp.where(inside, cumulative[..., :, None] - cumulative[..., None, :], -jnp.inf)
    )
    likeness = jnp.einsum("hid,hjd->hij", keys, keys, precision=HIGH)
    asked = jnp.einsum("hid,hjd->hij", queries, keys, precision=HIGH)
    strict = jnp.where(proper, likeness * decay * beta[..., None], 0.0)
    inverse = inverse_unit_triangular(strict)
    lift = jnp.exp(cumulative)[..., None]
    right = jnp.concatenate(
        [values * beta[..., None], keys * (beta[..., None] * lift)], axis=-1
    )
    solved = jnp.matmul(inverse, right, precision=HIGH)
    within = asked * decay
    keys_decayed = keys * jnp.exp(total - cumulative)[..., None]
    seen = jnp.matmul(within, solved, precision=HIGH)
    kept = jnp.einsum("ghti,ghtj->ghji", keys_decayed, solved, precision=HIGH)
    dv = values.shape[-1]
    start = jnp.sum(seen[..., :dv], axis=0)
    reach = queries * lift - seen[..., dv:]
    return start, reach, kept, total


def relay_kernel(n, per_direction, dk, maps_ref, out_ref):
    backward = lax.axis_index("sp") >= per_direction
    state = jnp.zeros(out_ref.shape[1:], jnp.float32)
    for step in range(n):
        at = jnp.where(backward, n - 1 - step, step)
        out_ref[at] = state.astype(out_ref.dtype)
        if step < n - 1:
            change = maps_ref[at, :dk, :]
            added = maps_ref[at, dk:, :].astype(jnp.float32)
            upper = state.astype(jnp.bfloat16)
            lower = (state - upper.astype(jnp.float32)).astype(jnp.bfloat16)
            moved = jnp.dot(upper, change, preferred_element_type=jnp.float32)
            moved = moved + jnp.dot(lower, change, preferred_element_type=jnp.float32)
            state = state + moved + added


def entering_states(change, added):
    n = lax.axis_size("sp")
    heads, dk = change.shape[1], change.shape[-1]
    dv = added.shape[2]
    share = n // (2 * heads)
    piece = dv // share
    maps = jnp.concatenate(
        [
            jnp.broadcast_to(change[:, :, None], (2, heads, share, dk, dk)),
            added.reshape(2, heads, share, piece, dk),
        ],
        axis=3,
    ).astype(jnp.bfloat16)
    maps = lax.all_to_all(maps.reshape(n, dk + piece, dk), "sp", 0, 0, tiled=True)
    states = pl.pallas_call(
        functools.partial(relay_kernel, n, n // 2, dk),
        out_shape=jax.ShapeDtypeStruct((n, piece, dk), jnp.bfloat16),
        in_specs=[pl.BlockSpec(memory_space=pltpu.VMEM)],
        out_specs=pl.BlockSpec(memory_space=pltpu.VMEM),
    )(maps)
    states = lax.all_to_all(states, "sp", 0, 0, tiled=True)
    return states.reshape(2, heads, dv, dk)


def gate_heads(mixture, result_valve_matrix, channel_scaling_vector):
    scaled = (
        mixture
        * lax.rsqrt(jnp.mean(mixture * mixture, axis=-1, keepdims=True) + 1e-06)
        * channel_scaling_vector
    )
    gated = scaled * jax.nn.silu(heads_of(result_valve_matrix, mixture.shape[-1]))
    return jnp.transpose(gated, (1, 0, 2)).reshape(gated.shape[1], -1).astype(jnp.bfloat16)


def rms_rows(rows, gain):
    widened = rows.astype(jnp.float32)
    return (
        widened * lax.rsqrt(jnp.mean(widened * widened, axis=-1, keepdims=True) + 1e-06) * gain
    ).astype(jnp.bfloat16)


def group_size(n):
    size = 1
    while 4 * size * size <= n:
        size = size * 2
    return size


def trade(pieces_for, stride, count):
    n = lax.axis_size("sp")
    place = lax.rem(lax.axis_index("sp") // stride, count)
    own = pieces_for(place)
    gathered = lax.dynamic_update_index_in_dim(
        jnp.zeros((count,) + own.shape, own.dtype), own, place, 0
    )
    for flip in range(1, count):
        other = lax.bitwise_xor(place, flip)
        route = [(s, s + ((((s // stride) % count) ^ flip) - (s // stride) % count) * stride) for s in range(n)]
        arrived = lax.ppermute(pieces_for(other), "sp", route)
        gathered = lax.dynamic_update_index_in_dim(gathered, arrived, other, 0)
    return gathered


def swap_within(array, dim, group):
    width = array.shape[dim] // group
    return trade(
        lambda member: lax.dynamic_slice_in_dim(array, member * width, width, axis=dim),
        1,
        group,
    )


def plain_body(
    skip_pathway,
    request_vectors,
    lookup_address_matrix,
    content_vectors,
    result_valve_matrix,
    shrink_raw_signal,
    channel_shrink_speed,
    insertion_raw_signal,
    extra_shrink_spike,
    channel_scaling_vector,
    final_mapping_matrix,
    mixer_scaling_vector,
    valve_matrix,
    widening_matrix,
    temporal_kernel_entries,
    narrowing_matrix,
):
    n = lax.axis_size("sp")
    group = group_size(n)
    place = lax.rem(lax.axis_index("sp"), group)
    far = [[o * group + i for o in range(n // group)] for i in range(group)]

    def collect(pieces):
        return lax.all_gather(pieces, "sp", axis=0, tiled=True, axis_index_groups=far)

    valve = swap_within(valve_matrix, 1, group)
    widening = swap_within(widening_matrix, 1, group)
    valve, widening, request_vectors, lookup_address_matrix = lax.optimization_barrier(
        (valve, widening, request_vectors, lookup_address_matrix)
    )
    valve = collect(valve)
    valve = valve.reshape(-1, valve.shape[-1])
    widening = collect(widening)
    widening = widening.reshape(-1, widening.shape[-1])
    narrowing = collect(swap_within(narrowing_matrix, 0, group))
    units = valve.shape[-1]
    taps = lax.dynamic_slice_in_dim(temporal_kernel_entries, place * units, units, axis=1)

    queries = unit_rows(heads_of(request_vectors, DK)) * DK ** (-0.5)
    keys = unit_rows(heads_of(lookup_address_matrix, DK))
    values = heads_of(content_vectors, DV)
    shrink_exponent = (
        -channel_shrink_speed[:, :, None] * jax.nn.softplus(shrink_raw_signal) + extra_shrink_spike
    )
    beta = jax.nn.sigmoid(insertion_raw_signal)
    start, reach, kept, total = local_parts(queries, keys, values, shrink_exponent, beta)
    added = kept[:, :, :DV]
    change = (
        jnp.expm1(total)[..., None] * jnp.eye(DK, dtype=jnp.float32) - kept[:, :, DV:]
    )
    states = entering_states(change, added)
    carried = jnp.einsum(
        "ghtk,ghvk->ghtv",
        reach.astype(jnp.bfloat16),
        states,
        preferred_element_type=jnp.float32,
    )
    mixture = start + carried[0] + carried[1]
    mixed = gate_heads(mixture, result_valve_matrix, channel_scaling_vector)
    projected = jnp.dot(
        lax.all_gather(mixed, "tp", axis=1, tiled=True),
        final_mapping_matrix,
        preferred_element_type=jnp.float32,
    )
    middle = (skip_pathway.astype(jnp.float32) + projected).astype(jnp.bfloat16)
    rows = trade(lambda member: middle, 1, group)
    full_rows = jnp.concatenate(
        [lax.all_gather(rows[i], "tp", axis=1, tiled=True) for i in range(group)], axis=0
    )
    normed = rms_rows(full_rows, mixer_scaling_vector)

    gate = jnp.dot(normed, valve, preferred_element_type=jnp.float32).astype(jnp.bfloat16)
    before = lax.ppermute(gate[-1:], "sp", [(s, s + group) for s in range(n - group)])
    after = lax.ppermute(gate[:1], "sp", [(s + group, s) for s in range(n - group)])
    up = jnp.dot(normed, widening, preferred_element_type=jnp.float32)
    padded = jnp.concatenate([before, gate, after], axis=0).astype(jnp.float32)
    convolved = padded[:-2] * taps[0] + padded[1:-1] * taps[1] + padded[2:] * taps[2]
    hidden = (jax.nn.silu(convolved) * up).astype(jnp.bfloat16)
    terms = jnp.einsum(
        "th,nhf->tnf", hidden, narrowing, preferred_element_type=jnp.float32
    ).reshape(hidden.shape[0], -1)
    summed = lax.psum_scatter(
        terms.astype(jnp.bfloat16), "tp", scatter_dimension=1, tiled=True
    )
    summed_parts = summed.reshape((group, -1) + summed.shape[1:])
    summed = trade(
        lambda member: lax.dynamic_index_in_dim(summed_parts, member, 0, keepdims=False),
        1,
        group,
    )
    summed = jnp.sum(summed.astype(jnp.float32), axis=0)
    return (middle.astype(jnp.float32) + summed).astype(jnp.bfloat16)


BF = jnp.bfloat16
F32 = jnp.float32
MESH = pl.DeviceIdType.MESH
EPS = 1e-06


def dot(a, b):
    return jnp.dot(a, b, preferred_element_type=F32)


def dot_last(a, b):
    return lax.dot_general(a, b, (((1,), (1,)), ((), ())), preferred_element_type=F32)


def dot_first(a, b):
    return lax.dot_general(a, b, (((0,), (0,)), ((), ())), preferred_element_type=F32)


def flipped(index, mask):
    result = index
    bit = 1
    while bit <= mask:
        if mask & bit:
            result = result + (1 - 2 * ((index // bit) % 2)) * bit
        bit = bit * 2
    return result


def carry_on(state, change):
    upper = state.astype(BF)
    lower = (state - upper.astype(F32)).astype(BF)
    return state + dot(upper, change) + dot(lower, change)


def silu(x):
    return x / (1.0 + jnp.exp(-x))


def only(when, act):
    if when is True:
        act()
    else:
        pl.when(when)(act)


class Flights:
    def __init__(self):
        self.sent = []

    def send(self, src, dst, send_sem, recv_sem, device, when=True):
        copy = pltpu.make_async_remote_copy(
            src_ref=src, dst_ref=dst, send_sem=send_sem, recv_sem=recv_sem,
            device_id=device, device_id_type=MESH,
        )
        only(when, copy.start)
        self.sent.append((when, copy))

    def finish(self):
        for when, copy in self.sent:
            only(when, copy.wait_send)


class Phases:
    def __init__(self):
        self.scope = None

    def __call__(self, name):
        if self.scope is not None:
            self.scope.__exit__(None, None, None)
        self.scope = jax.named_scope(name) if name else None
        if name:
            self.scope.__enter__()


def landed(dst, send_sem, recv_sem, device):
    pltpu.make_async_remote_copy(
        src_ref=dst, dst_ref=dst, send_sem=send_sem, recv_sem=recv_sem,
        device_id=device, device_id_type=MESH,
    ).wait_recv()


def layer_kernel(
    n, group,
    skip_any, q_any, k_any, v_any, z_any, shrink_any, speed_any, insert_any, spike_any,
    head_gain_any, fm_ref, row_gain_any, valve_ref, widening_ref, taps_any, narrowing_ref,
    out_ref,
    skip_ref, q_ref, k_ref, v_ref, z_ref, shrink_ref, speed_ref, insert_ref, spike_ref,
    head_gain_ref, row_gain_ref, taps_ref, staged_sem,
    fm, wv, wu, wn, maps_out, maps_in, tot_out, tot_in, st_out, st_in, reach, start, mixbuf,
    tok, nrm, edge_out, edge_in, halo, hid, x_out, x_in, mine, z_out, z_in,
    local_sem, wz_send, wz_recv, wp_send, wp_recv, map_send, map_recv, tot_send, tot_recv,
    st_send, st_recv, mix_send, mix_recv, edge_send, edge_recv, tok_send, tok_recv,
    halo_send, halo_recv, half_send, half_recv, hh_send, hh_recv, x_send, x_recv, z_send, z_recv,
):
    G, F = group, n // group
    nb = F.bit_length() - 1
    length, feats = skip_ref.shape
    heads = q_ref.shape[1] // DK
    units = wv.shape[2]
    cols = narrowing_ref.shape[1]
    s, t = lax.axis_index("sp"), lax.axis_index("tp")
    o, i = s // F, s % F
    other = 1 - t
    after, before = (s + 1) % n, (s + n - 1) % n
    flights = Flights()
    phase = Phases()

    def level(r):
        return flipped(o, r)

    barrier = pltpu.get_barrier_semaphore()
    peers = [(s, other), (after, t), (before, t)]
    peers += [(level(r) * F + i, t) for r in range(1, G)]
    peers += [(o * F + (i + r) % F, t) for r in range(1, F)]
    for peer in peers:
        pl.semaphore_signal(barrier, inc=1, device_id=peer, device_id_type=MESH)

    sources = (valve_ref, widening_ref, narrowing_ref)

    whole = (0, 1)

    def piece(w, lev, share=whole):
        e, of = share
        if w < 2:
            deep = valve_ref.shape[0] // of
            return sources[w].at[pl.ds(e * deep, deep), pl.ds(pl.multiple_of(lev * units, 128), units)]
        deep = units // of
        return sources[w].at[pl.ds(pl.multiple_of(lev * units + e * deep, 16), deep), :]

    def place(w, block, share=whole):
        e, of = share
        if w < 2:
            deep = valve_ref.shape[0] // of
            return (wv, wu)[w].at[block, pl.ds(e * deep, deep)]
        deep = units // of
        return wn.at[pl.ds(e * deep, deep), pl.ds(pl.multiple_of(block * cols, 128), cols)]

    early = [
        (speed_any, speed_ref), (shrink_any, shrink_ref), (spike_any, spike_ref), (insert_any, insert_ref),
        (k_any, k_ref), (q_any, q_ref), (v_any, v_ref),
    ]
    late = [
        (z_any, z_ref), (head_gain_any, head_gain_ref), (skip_any, skip_ref),
        (row_gain_any, row_gain_ref), (taps_any, taps_ref),
    ]
    staged = [
        pltpu.make_async_copy(src, dst, staged_sem.at[at]) for at, (src, dst) in enumerate(early + late)
    ]
    for copy in staged:
        copy.start()
    local = [pltpu.make_async_copy(fm_ref, fm, local_sem.at[3])]
    local += [pltpu.make_async_copy(piece(w, o), place(w, s), local_sem.at[w]) for w in range(3)]
    for copy in local:
        copy.start()
    phase("barrier")
    pl.semaphore_wait(barrier, len(peers))

    def swap(w, some=range(1, G)):
        for r in some:
            lev = level(r)
            at = w * G + r
            flights.send(piece(w, lev), place(w, s), wz_send.at[at], wz_recv.at[at], (lev * F + i, t))

    def wait_swap(w, d):
        at = w * G + d
        landed(place(w, level(d) * F + i), wz_send.at[at], wz_recv.at[at], (s, other))

    def order(e):
        return [1 << ((e + j) % nb) for j in range(nb)]

    def wait_spread(w, d, e, mask):
        at = ((w * G + d) * nb + e) * F + mask
        landed(
            place(w, level(d) * F + flipped(i, mask), (e, nb)), wp_send.at[at], wp_recv.at[at], (s, other)
        )

    def spread(w, d, stage):
        if stage == 0 and d > 0:
            wait_swap(w, d)
        for e in range(nb):
            bits = order(e)
            held = [0]
            for b in bits[:stage]:
                held = held + [m + b for m in held]
            for m in held:
                if stage > 0 and m & bits[stage - 1]:
                    wait_spread(w, d, e, m)
            for m in held:
                dst = place(w, level(d) * F + flipped(i, m), (e, nb))
                src = piece(w, o, (e, nb)) if m == 0 and d == 0 else dst
                at = ((w * G + d) * nb + e) * F + m + bits[stage]
                flights.send(src, dst, wp_send.at[at], wp_recv.at[at], (o * F + flipped(i, bits[stage]), t))

    def wait_last(w, d):
        for e in range(nb):
            for m in range(1, F):
                if m & order(e)[nb - 1]:
                    wait_spread(w, d, e, m)

    def wait_weights(w):
        local[1 + w].wait()
        for d in range(G):
            wait_last(w, d)

    phase("first_sends")
    swap(0)
    for w in range(2):
        spread(w, 0, 0)
    tot_in[o] = jnp.zeros(tot_in.shape[1:], BF)

    phase("setup")
    for copy in staged[: len(early)]:
        copy.wait()
    row = lax.broadcasted_iota(jnp.int32, (length, length), 0)
    column = lax.broadcasted_iota(jnp.int32, (length, length), 1)
    identity = jnp.where(row == column, 1.0, 0.0).astype(F32)
    R = 2 * heads
    which = lax.broadcasted_iota(jnp.int32, (R, length), 0)
    lane = lax.broadcasted_iota(jnp.int32, (R, length), 1)
    speed = jnp.zeros((R, length), F32)
    for g in range(2):
        for h in range(heads):
            speed = jnp.where(which == g * heads + h, speed_ref[g, h], speed)

    def both(ref):
        return jnp.concatenate([ref[0], ref[1]], axis=0)

    raw = both(shrink_ref)
    softplus = jnp.maximum(raw, 0.0) + jnp.log(1.0 + jnp.exp(-jnp.abs(raw)))
    total_c = both(spike_ref) - speed * softplus
    step = 1
    while step < length:
        ahead = jnp.where(lane >= step, pltpu.roll(total_c, step, 1), 0.0)
        behind = jnp.where(lane < length - step, pltpu.roll(total_c, length - step, 1), 0.0)
        total_c = total_c + jnp.where(which < heads, ahead, behind)
        step = step * 2
    cum = total_c
    total = jnp.where(which[:, :1] < heads, cum[:, length - 1 :], cum[:, :1])
    beta = 1.0 / (1.0 + jnp.exp(-both(insert_ref)))
    pad = jnp.zeros((length - 2 * R, length), F32)
    turned = jnp.transpose(jnp.concatenate([cum, beta, pad], axis=0))

    inside = (column <= row, column >= row)
    proper = (column < row, column > row)

    def crossing(b, g):
        near = row // (2 * b) == column // (2 * b)
        low = ((row // b) % 2 == 1) & ((column // b) % 2 == 0)
        high = ((row // b) % 2 == 0) & ((column // b) % 2 == 1)
        return near & (low if g == 0 else high)

    batch = min(heads, 2)
    for first in range(0, heads, batch):
        phase("local_attention")
        some = range(first, first + batch)
        problems = [(h, g) for h in some for g in range(2)]
        keys, queries, keys_b, like, asked = {}, {}, {}, {}, {}
        for h in some:
            k = k_ref[:, h * DK : (h + 1) * DK].astype(F32)
            q = q_ref[:, h * DK : (h + 1) * DK].astype(F32)
            keys[h] = k * lax.rsqrt(jnp.sum(k * k, axis=-1, keepdims=True) + EPS)
            queries[h] = q * (lax.rsqrt(jnp.sum(q * q, axis=-1, keepdims=True) + EPS) * DK ** (-0.5))
            keys_b[h] = keys[h].astype(BF)
            like[h] = dot_last(keys_b[h], keys_b[h])
            asked[h] = dot_last(queries[h].astype(BF), keys_b[h])
        cum_col, beta_col, decay, strict, inverse = {}, {}, {}, {}, {}
        for p in problems:
            h, g = p
            r = g * heads + h
            cum_col[p] = turned[:, r : r + 1]
            beta_col[p] = turned[:, R + r : R + r + 1]
            gap = jnp.where(inside[g], cum_col[p] - cum[r : r + 1, :], -1e30)
            decay[p] = jnp.exp(gap)
            strict[p] = jnp.where(proper[g], like[h] * decay[p] * beta_col[p], 0.0)
            inverse[p] = identity - jnp.where(crossing(1, g), strict[p], 0.0)
        b = 2
        while b < length:
            half, part = {}, {}
            for p in problems:
                half[p] = inverse[p].astype(BF)
                part[p] = jnp.where(crossing(b, p[1]), strict[p], 0.0).astype(BF)
            for p in problems:
                part[p] = dot(part[p], half[p]).astype(BF)
            for p in problems:
                inverse[p] = inverse[p] - dot(half[p], part[p])
            b = b * 2
        solved = {}
        for p in problems:
            h, g = p
            v = v_ref[:, h * DV : (h + 1) * DV].astype(F32)
            lift = jnp.exp(cum_col[p])
            right = jnp.concatenate(
                [(v * beta_col[p]).astype(BF), (keys[h] * (beta_col[p] * lift)).astype(BF)], axis=-1
            )
            solved[p] = dot(inverse[p].astype(BF), right).astype(BF)
        for p in problems:
            h, g = p
            r = g * heads + h
            lift = jnp.exp(cum_col[p])
            seen = dot((asked[h] * decay[p]).astype(BF), solved[p])
            reach[h, :, g * DK : (g + 1) * DK] = (queries[h] * lift - seen[:, DV:]).astype(BF)
            if g == 0:
                start[h] = seen[:, :DV]
            else:
                start[h] = start[h] + seen[:, :DV]
            fading = keys[h] * jnp.exp(total[r : r + 1, :] - cum_col[p])
            kept = dot_first(solved[p], fading.astype(BF))
            maps_out[h, g, :DK] = (identity * (jnp.exp(total[r : r + 1, :]) - 1.0) - kept[DV:]).astype(BF)
            maps_out[h, g, DK:] = kept[:DV].astype(BF)
        phase("send_maps")
        for h in some:
            flights.send(
                maps_out.at[h], maps_in.at[i], map_send.at[h], map_recv.at[i], (o * F + h, t), when=i != h
            )

            @pl.when(i == h)
            def _():
                maps_in[h] = maps_out[h]

    phase("spread_own")
    for w in range(2):
        spread(w, 0, 1)
    spread(2, 0, 0)

    phase("wait_maps")
    for j in range(F):

        @pl.when(i != j)
        def _():
            landed(maps_in.at[j], map_send.at[j], map_recv.at[j], (s, other))

    phase("compose")
    def turn(g, j):
        return j if g == 0 else F - 1 - j

    whole_maps = []
    for g in range(2):
        whole_maps.append(maps_in[turn(g, 0), g].astype(F32))
    for j in range(1, F):
        for g in range(2):
            at = turn(g, j)
            whole_maps[g] = carry_on(whole_maps[g], maps_in[at, g, :DK]) + maps_in[at, g].astype(F32)
    for g in range(2):
        tot_out[g] = whole_maps[g].astype(BF)
    phase("send_totals")
    for r in range(1, G):
        flights.send(
            tot_out.at[(o // (1 << (r.bit_length() - 1))) % 2], tot_in.at[o], tot_send.at[r], tot_recv.at[r], (level(r) * F + i, t)
        )
    phase("spread_0_0")
    for d in range(1, G):
        spread(0, d, 0)
    phase("wait_totals")
    for r in range(1, G):
        landed(tot_in.at[level(r)], tot_send.at[r], tot_recv.at[r], (s, other))
    swap(1)
    phase("states")
    states = [jnp.zeros((DV, DK), F32) for _ in range(2)]
    for j in range(G - 1):
        for g in range(2):
            at = j if g == 0 else G - 1 - j
            counts = (at < o) if g == 0 else (at > o)
            m = jnp.where(counts, tot_in[at].astype(F32), 0.0)
            states[g] = carry_on(states[g], m[:DK].astype(BF)) + m[DK:]
    for j in range(F):
        for g in range(2):
            at = turn(g, j)
            st_out[at, :, g * DK : (g + 1) * DK] = states[g].astype(BF)
            if j < F - 1:
                states[g] = carry_on(states[g], maps_in[at, g, :DK]) + maps_in[at, g, DK:].astype(F32)
    phase("send_states")
    for r in range(1, F):
        to = (i + r) % F
        flights.send(st_out.at[to], st_in.at[i], st_send.at[r], st_recv.at[r], (o * F + to, t))
    st_in[i] = st_out[i]
    spread(2, 0, 1)
    phase("wait_states")
    for r in range(1, F):
        landed(st_in.at[(i + F - r) % F], st_send.at[r], st_recv.at[r], (s, other))

    phase("outputs")
    for copy in staged[len(early) :]:
        copy.wait()
    for h in range(heads):
        mixture = start[h] + dot_last(reach[h], st_in[h])
        scale = lax.rsqrt(jnp.mean(mixture * mixture, axis=-1, keepdims=True) + EPS)
        valve = z_ref[:, h * DV : (h + 1) * DV].astype(F32)
        gated = mixture * scale * head_gain_ref[...] * silu(valve)
        mixbuf[t, :, h * DV : (h + 1) * DV] = gated.astype(BF)
    flights.send(mixbuf.at[t], mixbuf.at[t], mix_send, mix_recv, (s, other))
    phase("spread_0_1")
    for d in range(1, G):
        spread(0, d, 1)
    phase("project")
    local[0].wait()
    wide = heads * DV
    projected = dot(mixbuf[t], fm[pl.ds(pl.multiple_of(t * wide, 128), wide), :])
    phase("wait_mix")
    landed(mixbuf.at[other], mix_send, mix_recv, (s, other))
    phase("middle")
    projected = projected + dot(mixbuf[other], fm[pl.ds(pl.multiple_of(other * wide, 128), wide), :])
    middle = (skip_ref[...].astype(F32) + projected).astype(BF)
    tok[o, t] = middle

    def share(block, when=True):
        flights.send(
            tok.at[block, t], tok.at[block, t], half_send.at[block], half_recv.at[block], (s, other), when=when
        )

    def pass_up(block, when):
        flights.send(
            tok.at[block, t], tok.at[block, t], tok_send.at[block], tok_recv.at[block],
            (s + F, t), when=when & (o < G - 1),
        )

    def pass_down(block, when):
        flights.send(
            tok.at[block, t], tok.at[block, t], tok_send.at[G + block], tok_recv.at[block],
            (s - F, t), when=when & (o > 0),
        )

    def arrive(distance):
        for below in (True, False):
            block = o - distance if below else o + distance
            there = block >= 0 if below else block < G

            @pl.when(there)
            def _():
                landed(tok.at[block, t], tok_send.at[block], tok_recv.at[block], (s, other))

            share(block, when=there)
            (pass_up if below else pass_down)(block, there)

    pass_up(o, o >= 0)
    pass_down(o, o >= 0)
    share(o)
    strips = feats // 128
    ends = jnp.concatenate([middle[:1], middle[length - 1 :]], axis=0).astype(F32)
    edge_out[...] = jnp.concatenate(
        [ends[e : e + 1, c * 128 : (c + 1) * 128] for e in range(2) for c in range(strips)], axis=0
    ).astype(BF)
    flights.send(edge_out, edge_in.at[0], edge_send.at[0], edge_recv.at[0], (after, t))
    flights.send(edge_out, edge_in.at[1], edge_send.at[1], edge_recv.at[1], (before, t))
    def normed(rows0, rows1):
        squares = jnp.sum(rows0 * rows0, axis=-1, keepdims=True) + jnp.sum(rows1 * rows1, axis=-1, keepdims=True)
        scale = lax.rsqrt(squares * (1.0 / (2 * feats)) + EPS)
        return (
            (rows0 * scale * row_gain_ref[:, :feats]).astype(BF),
            (rows1 * scale * row_gain_ref[:, feats:]).astype(BF),
        )

    def strip_rows(block, half):
        rows = []
        for side in range(2):
            packed = halo[block, half, side].astype(F32)
            base = (1 - side) * strips
            rows.append(jnp.concatenate([packed[base + c : base + c + 1] for c in range(strips)], axis=1))
        return jnp.concatenate(rows + [jnp.zeros((14, feats), F32)], axis=0)

    my_taps = taps_ref[:, pl.ds(pl.multiple_of(o * units, 128), units)]
    row_u = lax.broadcasted_iota(jnp.int32, (length, units), 0)

    def work(r):
        block = flipped(o, r)
        if r > 0:
            phase("relay_halo")
            landed(halo.at[block, t], halo_send.at[r], halo_recv.at[block], (s, other))
            flights.send(
                halo.at[block, t], halo.at[block, t], hh_send.at[block], hh_recv.at[block], (s, other)
            )
        phase("wait_rows_from_core")
        landed(tok.at[block, other], half_send.at[block], half_recv.at[block], (s, other))
        landed(halo.at[block, other], hh_send.at[block], hh_recv.at[block], (s, other))
        phase("ffn_in")
        a, b2 = normed(tok[block, 0].astype(F32), tok[block, 1].astype(F32))
        nrm[:length, :feats] = a
        nrm[:length, feats:] = b2
        a, b2 = normed(strip_rows(block, 0), strip_rows(block, 1))
        nrm[length:, :feats] = a
        nrm[length:, feats:] = b2
        gate = dot(nrm[...], wv[...].reshape(2 * feats, units)).astype(BF).astype(F32)
        up = dot(nrm[:length], wu[...].reshape(2 * feats, units))
        at = block * F + i
        first_row = jnp.where(at > 0, gate[length : length + 1], 0.0)
        last_row = jnp.where(at < n - 1, gate[length + 1 : length + 2], 0.0)
        here = gate[:length]
        earlier = jnp.where(row_u == 0, first_row, pltpu.roll(here, 1, 0))
        later = jnp.where(row_u == length - 1, last_row, pltpu.roll(here, length - 1, 0))
        convolved = earlier * my_taps[0:1] + here * my_taps[1:2] + later * my_taps[2:3]
        hid[r] = (silu(convolved) * up).astype(BF)

    parts = G // 2
    chunk = F * cols

    def down(d, some):
        first, size = some
        lev = level(d)
        home, q = lev // parts, lev % parts
        rows = pl.ds(first, size)
        product = dot(
            hid[rows].reshape(size * length, units), wn[:, pl.ds(pl.multiple_of(lev * chunk, 128), chunk)]
        )

        @pl.when(home != t)
        def _():
            x_out[q, rows] = product.astype(BF).reshape(size, length, chunk)

        flights.send(
            x_out.at[q, rows], x_in.at[q, rows], x_send.at[q * G + first], x_recv.at[q * G + first],
            (s, other), when=home != t,
        )

        @pl.when(home == t)
        def _():
            mine[q, rows] = product.astype(BF).reshape(size, length, chunk)

    def settle(d, some):
        first, size = some
        lev = level(d)
        home, q = lev // parts, lev % parts
        rows = pl.ds(first, size)

        @pl.when(home == t)
        def _():
            landed(x_in.at[q, rows], x_send.at[q * G + first], x_recv.at[q * G + first], (s, other))
            z_out[q, rows] = (mine[q, rows].astype(F32) + x_in[q, rows].astype(F32)).astype(BF)

        for r in range(max(first, 1), first + size):
            flights.send(
                z_out.at[q, r], z_in.at[o, q], z_send.at[q * G + r], z_recv.at[o * parts + q],
                (level(r) * F + i, t), when=home == t,
            )

    swap(2, [1])
    phase("spread_1_0")
    for d in range(1, G):
        spread(1, d, 0)
    phase("rows_1")
    arrive(1)
    swap(2, range(2, G))
    phase("spread_1_1")
    for d in range(1, G):
        spread(1, d, 1)
    phase("wait_edges")
    landed(edge_in.at[0], edge_send.at[0], edge_recv.at[0], (s, other))
    landed(edge_in.at[1], edge_send.at[1], edge_recv.at[1], (s, other))
    halo[o, t] = edge_in[...]
    for r in range(1, G):
        flights.send(edge_in, halo.at[o, t], halo_send.at[r], halo_recv.at[o], (level(r) * F + i, t))
    flights.send(edge_in, halo.at[o, t], hh_send.at[o], hh_recv.at[o], (s, other))
    phase("spread_2_0")
    spread(2, 1, 0)
    for distance in range(2, G - 1):
        phase("rows_2")
        arrive(distance)
    phase("wait_weights")
    wait_weights(0)
    wait_weights(1)
    near, far, every = (0, G // 2), (G // 2, G // 2), (0, G)
    for r in range(G // 2):
        work(r)
    phase("spread_2_0")
    for d in range(2, G):
        spread(2, d, 0)
    spread(2, 1, 1)
    phase("down_own")
    wait_last(2, 0)
    local[3].wait()
    down(0, near)
    phase("rows_3")
    arrive(G - 1)
    phase("settle_own")
    settle(0, near)
    for r in range(G // 2, G):
        work(r)
    phase("spread_2_1")
    for d in range(2, G):
        spread(2, d, 1)
    phase("down_own")
    down(0, far)
    settle(0, far)
    for d in range(1, G):
        phase("wait_narrowing")
        wait_last(2, d)
        phase("down")
        down(d, every)
        phase("settle")
        settle(d, every)
    phase("result")
    for q in range(parts):
        at = slice(q * chunk, (q + 1) * chunk)
        result = tok[o, t, :, at].astype(F32) + z_out[q, 0].astype(F32)
        for r in range(1, G):
            lev = level(r)
            landed(z_in.at[lev, q], z_send.at[q], z_recv.at[lev * parts + q], (s, other))
            result = result + z_in[lev, q].astype(F32)
        out_ref[:, at] = result.astype(BF)

    phase("finish")
    flights.finish()

    phase(None)


def fits(n, tp, length, feats, heads, units, rows, cols):
    group = group_size(n)
    far = n // group
    return (
        tp == 2 and group > 1 and far == heads and far & (far - 1) == 0 and heads % 2 == 0
        and length == DK and DK == DV and feats % 128 == 0
        and units % group == 0 and (units // group) % 128 == 0 and cols % 128 == 0 and rows % 16 == 0
    )


def fused_body(
    skip_pathway, request_vectors, lookup_address_matrix, content_vectors, result_valve_matrix,
    shrink_raw_signal, channel_shrink_speed, insertion_raw_signal, extra_shrink_spike,
    channel_scaling_vector, final_mapping_matrix, mixer_scaling_vector, valve_matrix,
    widening_matrix, temporal_kernel_entries, narrowing_matrix,
):
    n = lax.axis_size("sp")
    G = group_size(n)
    F = n // G
    length, feats = skip_pathway.shape
    heads = request_vectors.shape[1] // DK
    rows = valve_matrix.shape[0]
    units = valve_matrix.shape[1] // G
    strips = feats // 128
    vmem, anywhere = pl.BlockSpec(memory_space=pltpu.VMEM), pl.BlockSpec(memory_space=pl.ANY)
    dma = pltpu.SemaphoreType.DMA
    head_gain = channel_scaling_vector.reshape(1, -1)
    row_gain = mixer_scaling_vector.reshape(1, -1)
    staged = [
        skip_pathway, request_vectors, lookup_address_matrix, content_vectors, result_valve_matrix,
        shrink_raw_signal, channel_shrink_speed, insertion_raw_signal, extra_shrink_spike,
        head_gain, row_gain, temporal_kernel_entries,
    ]
    stages = [
        pltpu.SMEM(x.shape, x.dtype) if x is channel_shrink_speed else pltpu.VMEM(x.shape, x.dtype)
        for x in staged
    ]
    return pl.pallas_call(
        functools.partial(layer_kernel, n, G),
        out_shape=jax.ShapeDtypeStruct((length, feats), BF),
        in_specs=[anywhere] * 16,
        out_specs=vmem,
        scratch_shapes=stages + [
            dma((len(staged),)),
            pltpu.VMEM(final_mapping_matrix.shape, BF),
            pltpu.VMEM((n, rows, units), BF),
            pltpu.VMEM((n, rows, units), BF),
            pltpu.VMEM((units, 2 * feats), BF),
            pltpu.VMEM((heads, 2, DK + DV, DK), BF),
            pltpu.VMEM((F, 2, DK + DV, DK), BF),
            pltpu.VMEM((2, DK + DV, DK), BF),
            pltpu.VMEM((G, DK + DV, DK), BF),
            pltpu.VMEM((F, DV, 2 * DK), BF),
            pltpu.VMEM((heads, DV, 2 * DK), BF),
            pltpu.VMEM((heads, length, 2 * DK), BF),
            pltpu.VMEM((heads, length, DV), F32),
            pltpu.VMEM((2, length, heads * DV), BF),
            pltpu.VMEM((G, 2, length, feats), BF),
            pltpu.VMEM((length + 16, 2 * feats), BF),
            pltpu.VMEM((2 * strips, 128), BF),
            pltpu.VMEM((2, 2 * strips, 128), BF),
            pltpu.VMEM((G, 2, 2, 2 * strips, 128), BF),
            pltpu.VMEM((G, length, units), BF),
            pltpu.VMEM((G // 2, G, length, 2 * feats // G), BF),
            pltpu.VMEM((G // 2, G, length, 2 * feats // G), BF),
            pltpu.VMEM((G // 2, G, length, 2 * feats // G), BF),
            pltpu.VMEM((G // 2, G, length, 2 * feats // G), BF),
            pltpu.VMEM((G, G // 2, length, 2 * feats // G), BF),
            dma((4,)),
            dma((3 * G,)), dma((3 * G,)),
            dma((3 * G * F * (F.bit_length() - 1),)), dma((3 * G * F * (F.bit_length() - 1),)),
            dma((F,)), dma((F,)),
            dma((G,)), dma((G,)),
            dma((F,)), dma((F,)),
            dma, dma,
            dma((2,)), dma((2,)),
            dma((2 * G,)), dma((G,)),
            dma((G,)), dma((G,)),
            dma((G,)), dma((G,)),
            dma((G,)), dma((G,)),
            dma((G * G // 2,)), dma((G * G // 2,)),
            dma((G * G // 2,)), dma((G * G // 2,)),
        ],
        compiler_params=pltpu.CompilerParams(
            collective_id=0, has_side_effects=True, vmem_limit_bytes=60 * 1024 * 1024
        ),
        name="layer",
    )(
        skip_pathway, request_vectors, lookup_address_matrix, content_vectors, result_valve_matrix,
        shrink_raw_signal, channel_shrink_speed, insertion_raw_signal, extra_shrink_spike,
        head_gain, final_mapping_matrix, row_gain,
        valve_matrix, widening_matrix, temporal_kernel_entries, narrowing_matrix,
    )


def body(*arrays):
    skip, queries = arrays[0], arrays[1]
    valve, narrowing = arrays[12], arrays[15]
    n, tp = lax.axis_size("sp"), lax.axis_size("tp")
    if fits(n, tp, *skip.shape, queries.shape[1] // DK, valve.shape[1], valve.shape[0], narrowing.shape[1]):
        return fused_body(*arrays)
    return plain_body(*arrays)


def solution(mesh):
    return jax.shard_map(
        body,
        mesh=mesh,
        in_specs=(
            P("sp", "tp"),
            P("sp", "tp"),
            P("sp", "tp"),
            P("sp", "tp"),
            P("sp", "tp"),
            P(None, "tp", "sp"),
            P(None, "tp"),
            P(None, "tp", "sp"),
            P(None, "tp", "sp"),
            P(),
            P(None, "tp"),
            P(),
            P("sp", "tp"),
            P("sp", "tp"),
            P(None, "tp"),
            P("tp", "sp"),
        ),
        out_specs=P("sp", "tp"),
        check_vma=False,
    )
```

```python
import functools

import jax
import jax.numpy as jnp
from jax import lax
from jax.experimental import pallas as pl
from jax.experimental.pallas import tpu as pltpu
from jax.sharding import PartitionSpec as P

DK = 128
DV = 128

HIGH = lax.Precision.HIGH


def heads_of(matrix, head_size):
    return jnp.transpose(
        matrix.astype(jnp.float32).reshape(matrix.shape[0], -1, head_size), (1, 0, 2)
    )


def unit_rows(vectors):
    return vectors * lax.rsqrt(jnp.sum(vectors * vectors, axis=-1, keepdims=True) + 1e-06)


def inverse_unit_triangular(strict):
    width = strict.shape[-1]
    identity = jnp.eye(width, dtype=jnp.float32)
    powered = -strict
    result = identity + powered
    covered = 2
    while covered < width:
        powered = jnp.matmul(powered, powered, precision=HIGH)
        result = result + jnp.matmul(result, powered, precision=HIGH)
        covered = covered * 2
    return result


def local_parts(queries, keys, values, shrink_exponent, beta):
    length = queries.shape[1]
    row = lax.broadcasted_iota(jnp.int32, (length, length), 0)
    column = lax.broadcasted_iota(jnp.int32, (length, length), 1)
    inside = jnp.stack([column <= row, column >= row])[:, None]
    proper = jnp.stack([column < row, column > row])[:, None]
    cumulative = jnp.sum(jnp.where(inside, shrink_exponent[:, :, None, :], 0.0), axis=-1)
    total = jnp.sum(shrink_exponent, axis=-1, keepdims=True)
    decay = jnp.exp(
        jnp.where(inside, cumulative[..., :, None] - cumulative[..., None, :], -jnp.inf)
    )
    likeness = jnp.einsum("hid,hjd->hij", keys, keys, precision=HIGH)
    asked = jnp.einsum("hid,hjd->hij", queries, keys, precision=HIGH)
    strict = jnp.where(proper, likeness * decay * beta[..., None], 0.0)
    inverse = inverse_unit_triangular(strict)
    lift = jnp.exp(cumulative)[..., None]
    right = jnp.concatenate(
        [values * beta[..., None], keys * (beta[..., None] * lift)], axis=-1
    )
    solved = jnp.matmul(inverse, right, precision=HIGH)
    within = asked * decay
    keys_decayed = keys * jnp.exp(total - cumulative)[..., None]
    seen = jnp.matmul(within, solved, precision=HIGH)
    kept = jnp.einsum("ghti,ghtj->ghji", keys_decayed, solved, precision=HIGH)
    dv = values.shape[-1]
    start = jnp.sum(seen[..., :dv], axis=0)
    reach = queries * lift - seen[..., dv:]
    return start, reach, kept, total


def relay_kernel(n, per_direction, dk, maps_ref, out_ref):
    backward = lax.axis_index("sp") >= per_direction
    state = jnp.zeros(out_ref.shape[1:], jnp.float32)
    for step in range(n):
        at = jnp.where(backward, n - 1 - step, step)
        out_ref[at] = state.astype(out_ref.dtype)
        if step < n - 1:
            change = maps_ref[at, :dk, :]
            added = maps_ref[at, dk:, :].astype(jnp.float32)
            upper = state.astype(jnp.bfloat16)
            lower = (state - upper.astype(jnp.float32)).astype(jnp.bfloat16)
            moved = jnp.dot(upper, change, preferred_element_type=jnp.float32)
            moved = moved + jnp.dot(lower, change, preferred_element_type=jnp.float32)
            state = state + moved + added


def entering_states(change, added):
    n = lax.axis_size("sp")
    heads, dk = change.shape[1], change.shape[-1]
    dv = added.shape[2]
    share = n // (2 * heads)
    piece = dv // share
    maps = jnp.concatenate(
        [
            jnp.broadcast_to(change[:, :, None], (2, heads, share, dk, dk)),
            added.reshape(2, heads, share, piece, dk),
        ],
        axis=3,
    ).astype(jnp.bfloat16)
    maps = lax.all_to_all(maps.reshape(n, dk + piece, dk), "sp", 0, 0, tiled=True)
    states = pl.pallas_call(
        functools.partial(relay_kernel, n, n // 2, dk),
        out_shape=jax.ShapeDtypeStruct((n, piece, dk), jnp.bfloat16),
        in_specs=[pl.BlockSpec(memory_space=pltpu.VMEM)],
        out_specs=pl.BlockSpec(memory_space=pltpu.VMEM),
    )(maps)
    states = lax.all_to_all(states, "sp", 0, 0, tiled=True)
    return states.reshape(2, heads, dv, dk)


def gate_heads(mixture, result_valve_matrix, channel_scaling_vector):
    scaled = (
        mixture
        * lax.rsqrt(jnp.mean(mixture * mixture, axis=-1, keepdims=True) + 1e-06)
        * channel_scaling_vector
    )
    gated = scaled * jax.nn.silu(heads_of(result_valve_matrix, mixture.shape[-1]))
    return jnp.transpose(gated, (1, 0, 2)).reshape(gated.shape[1], -1).astype(jnp.bfloat16)


def rms_rows(rows, gain):
    widened = rows.astype(jnp.float32)
    return (
        widened * lax.rsqrt(jnp.mean(widened * widened, axis=-1, keepdims=True) + 1e-06) * gain
    ).astype(jnp.bfloat16)


def group_size(n):
    size = 1
    while 4 * size * size <= n:
        size = size * 2
    return size


def trade(pieces_for, stride, count):
    n = lax.axis_size("sp")
    place = lax.rem(lax.axis_index("sp") // stride, count)
    own = pieces_for(place)
    gathered = lax.dynamic_update_index_in_dim(
        jnp.zeros((count,) + own.shape, own.dtype), own, place, 0
    )
    for flip in range(1, count):
        other = lax.bitwise_xor(place, flip)
        route = [(s, s + ((((s // stride) % count) ^ flip) - (s // stride) % count) * stride) for s in range(n)]
        arrived = lax.ppermute(pieces_for(other), "sp", route)
        gathered = lax.dynamic_update_index_in_dim(gathered, arrived, other, 0)
    return gathered


def swap_within(array, dim, group):
    width = array.shape[dim] // group
    return trade(
        lambda member: lax.dynamic_slice_in_dim(array, member * width, width, axis=dim),
        1,
        group,
    )


def plain_body(
    skip_pathway,
    request_vectors,
    lookup_address_matrix,
    content_vectors,
    result_valve_matrix,
    shrink_raw_signal,
    channel_shrink_speed,
    insertion_raw_signal,
    extra_shrink_spike,
    channel_scaling_vector,
    final_mapping_matrix,
    mixer_scaling_vector,
    valve_matrix,
    widening_matrix,
    temporal_kernel_entries,
    narrowing_matrix,
):
    n = lax.axis_size("sp")
    group = group_size(n)
    place = lax.rem(lax.axis_index("sp"), group)
    far = [[o * group + i for o in range(n // group)] for i in range(group)]

    def collect(pieces):
        return lax.all_gather(pieces, "sp", axis=0, tiled=True, axis_index_groups=far)

    valve = swap_within(valve_matrix, 1, group)
    widening = swap_within(widening_matrix, 1, group)
    valve, widening, request_vectors, lookup_address_matrix = lax.optimization_barrier(
        (valve, widening, request_vectors, lookup_address_matrix)
    )
    valve = collect(valve)
    valve = valve.reshape(-1, valve.shape[-1])
    widening = collect(widening)
    widening = widening.reshape(-1, widening.shape[-1])
    narrowing = collect(swap_within(narrowing_matrix, 0, group))
    units = valve.shape[-1]
    taps = lax.dynamic_slice_in_dim(temporal_kernel_entries, place * units, units, axis=1)

    queries = unit_rows(heads_of(request_vectors, DK)) * DK ** (-0.5)
    keys = unit_rows(heads_of(lookup_address_matrix, DK))
    values = heads_of(content_vectors, DV)
    shrink_exponent = (
        -channel_shrink_speed[:, :, None] * jax.nn.softplus(shrink_raw_signal) + extra_shrink_spike
    )
    beta = jax.nn.sigmoid(insertion_raw_signal)
    start, reach, kept, total = local_parts(queries, keys, values, shrink_exponent, beta)
    added = kept[:, :, :DV]
    change = (
        jnp.expm1(total)[..., None] * jnp.eye(DK, dtype=jnp.float32) - kept[:, :, DV:]
    )
    states = entering_states(change, added)
    carried = jnp.einsum(
        "ghtk,ghvk->ghtv",
        reach.astype(jnp.bfloat16),
        states,
        preferred_element_type=jnp.float32,
    )
    mixture = start + carried[0] + carried[1]
    mixed = gate_heads(mixture, result_valve_matrix, channel_scaling_vector)
    projected = jnp.dot(
        lax.all_gather(mixed, "tp", axis=1, tiled=True),
        final_mapping_matrix,
        preferred_element_type=jnp.float32,
    )
    middle = (skip_pathway.astype(jnp.float32) + projected).astype(jnp.bfloat16)
    rows = trade(lambda member: middle, 1, group)
    full_rows = jnp.concatenate(
        [lax.all_gather(rows[i], "tp", axis=1, tiled=True) for i in range(group)], axis=0
    )
    normed = rms_rows(full_rows, mixer_scaling_vector)

    gate = jnp.dot(normed, valve, preferred_element_type=jnp.float32).astype(jnp.bfloat16)
    before = lax.ppermute(gate[-1:], "sp", [(s, s + group) for s in range(n - group)])
    after = lax.ppermute(gate[:1], "sp", [(s + group, s) for s in range(n - group)])
    up = jnp.dot(normed, widening, preferred_element_type=jnp.float32)
    padded = jnp.concatenate([before, gate, after], axis=0).astype(jnp.float32)
    convolved = padded[:-2] * taps[0] + padded[1:-1] * taps[1] + padded[2:] * taps[2]
    hidden = (jax.nn.silu(convolved) * up).astype(jnp.bfloat16)
    terms = jnp.einsum(
        "th,nhf->tnf", hidden, narrowing, preferred_element_type=jnp.float32
    ).reshape(hidden.shape[0], -1)
    summed = lax.psum_scatter(
        terms.astype(jnp.bfloat16), "tp", scatter_dimension=1, tiled=True
    )
    summed_parts = summed.reshape((group, -1) + summed.shape[1:])
    summed = trade(
        lambda member: lax.dynamic_index_in_dim(summed_parts, member, 0, keepdims=False),
        1,
        group,
    )
    summed = jnp.sum(summed.astype(jnp.float32), axis=0)
    return (middle.astype(jnp.float32) + summed).astype(jnp.bfloat16)


BF = jnp.bfloat16
F32 = jnp.float32
MESH = pl.DeviceIdType.MESH
EPS = 1e-06


def dot(a, b):
    return jnp.dot(a, b, preferred_element_type=F32)


def dot_last(a, b):
    return lax.dot_general(a, b, (((1,), (1,)), ((), ())), preferred_element_type=F32)


def dot_first(a, b):
    return lax.dot_general(a, b, (((0,), (0,)), ((), ())), preferred_element_type=F32)


def flipped(index, mask):
    result = index
    bit = 1
    while bit <= mask:
        if mask & bit:
            result = result + (1 - 2 * ((index // bit) % 2)) * bit
        bit = bit * 2
    return result


def carry_on(state, change):
    upper = state.astype(BF)
    lower = (state - upper.astype(F32)).astype(BF)
    return state + dot(upper, change) + dot(lower, change)


def silu(x):
    return x / (1.0 + jnp.exp(-x))


def only(when, act):
    if when is True:
        act()
    else:
        pl.when(when)(act)


class Flights:
    def __init__(self):
        self.sent = []

    def send(self, src, dst, send_sem, recv_sem, device, when=True):
        copy = pltpu.make_async_remote_copy(
            src_ref=src, dst_ref=dst, send_sem=send_sem, recv_sem=recv_sem,
            device_id=device, device_id_type=MESH,
        )
        only(when, copy.start)
        self.sent.append((when, copy))

    def finish(self):
        for when, copy in self.sent:
            only(when, copy.wait_send)


class Phases:
    def __init__(self):
        self.scope = None

    def __call__(self, name):
        if self.scope is not None:
            self.scope.__exit__(None, None, None)
        self.scope = jax.named_scope(name) if name else None
        if name:
            self.scope.__enter__()


def landed(dst, send_sem, recv_sem, device):
    pltpu.make_async_remote_copy(
        src_ref=dst, dst_ref=dst, send_sem=send_sem, recv_sem=recv_sem,
        device_id=device, device_id_type=MESH,
    ).wait_recv()


def layer_kernel(
    n, group,
    skip_any, q_any, k_any, v_any, z_any, shrink_any, speed_any, insert_any, spike_any,
    head_gain_any, fm_ref, row_gain_any, valve_ref, widening_ref, taps_any, narrowing_ref,
    out_ref,
    skip_ref, q_ref, k_ref, v_ref, z_ref, shrink_ref, speed_ref, insert_ref, spike_ref,
    head_gain_ref, row_gain_ref, taps_ref, staged_sem,
    fm, wv, wu, wn, maps_out, maps_in, tot_out, tot_in, st_out, st_in, reach, start, mixbuf,
    tok, nrm, edge_out, edge_in, halo, hid, x_out, x_in, mine, z_out, z_in,
    local_sem, wz_send, wz_recv, wp_send, wp_recv, map_send, map_recv, tot_send, tot_recv,
    st_send, st_recv, mix_send, mix_recv, edge_send, edge_recv, tok_send, tok_recv,
    halo_send, halo_recv, half_send, half_recv, hh_send, hh_recv, x_send, x_recv, z_send, z_recv,
):
    G, F = group, n // group
    nb = F.bit_length() - 1
    length, feats = skip_ref.shape
    heads = q_ref.shape[1] // DK
    units = wv.shape[2]
    cols = narrowing_ref.shape[1]
    s, t = lax.axis_index("sp"), lax.axis_index("tp")
    o, i = s // F, s % F
    other = 1 - t
    after, before = (s + 1) % n, (s + n - 1) % n
    flights = Flights()
    phase = Phases()

    def level(r):
        return flipped(o, r)

    barrier = pltpu.get_barrier_semaphore()
    peers = [(s, other), (after, t), (before, t)]
    peers += [(level(r) * F + i, t) for r in range(1, G)]
    peers += [(o * F + (i + r) % F, t) for r in range(1, F)]
    for peer in peers:
        pl.semaphore_signal(barrier, inc=1, device_id=peer, device_id_type=MESH)

    sources = (valve_ref, widening_ref, narrowing_ref)

    whole = (0, 1)

    def piece(w, lev, share=whole):
        e, of = share
        if w < 2:
            deep = valve_ref.shape[0] // of
            return sources[w].at[pl.ds(e * deep, deep), pl.ds(pl.multiple_of(lev * units, 128), units)]
        deep = units // of
        return sources[w].at[pl.ds(pl.multiple_of(lev * units + e * deep, 16), deep), :]

    def place(w, block, share=whole):
        e, of = share
        if w < 2:
            deep = valve_ref.shape[0] // of
            return (wv, wu)[w].at[block, pl.ds(e * deep, deep)]
        deep = units // of
        return wn.at[pl.ds(e * deep, deep), pl.ds(pl.multiple_of(block * cols, 128), cols)]

    early = [
        (speed_any, speed_ref), (shrink_any, shrink_ref), (spike_any, spike_ref), (insert_any, insert_ref),
        (k_any, k_ref), (q_any, q_ref), (v_any, v_ref),
    ]
    late = [
        (z_any, z_ref), (head_gain_any, head_gain_ref), (skip_any, skip_ref),
        (row_gain_any, row_gain_ref), (taps_any, taps_ref),
    ]
    staged = [
        pltpu.make_async_copy(src, dst, staged_sem.at[at]) for at, (src, dst) in enumerate(early + late)
    ]
    for copy in staged:
        copy.start()
    local = [pltpu.make_async_copy(fm_ref, fm, local_sem.at[3])]
    local += [pltpu.make_async_copy(piece(w, o), place(w, s), local_sem.at[w]) for w in range(3)]
    for copy in local:
        copy.start()
    phase("barrier")
    pl.semaphore_wait(barrier, len(peers))

    def swap(w, some=range(1, G)):
        for r in some:
            lev = level(r)
            at = w * G + r
            flights.send(piece(w, lev), place(w, s), wz_send.at[at], wz_recv.at[at], (lev * F + i, t))

    def wait_swap(w, d):
        at = w * G + d
        landed(place(w, level(d) * F + i), wz_send.at[at], wz_recv.at[at], (s, other))

    def order(e):
        return [1 << ((e + j) % nb) for j in range(nb)]

    def wait_spread(w, d, e, mask):
        at = ((w * G + d) * nb + e) * F + mask
        landed(
            place(w, level(d) * F + flipped(i, mask), (e, nb)), wp_send.at[at], wp_recv.at[at], (s, other)
        )

    def spread(w, d, stage):
        if stage == 0 and d > 0:
            wait_swap(w, d)
        for e in range(nb):
            bits = order(e)
            held = [0]
            for b in bits[:stage]:
                held = held + [m + b for m in held]
            for m in held:
                if stage > 0 and m & bits[stage - 1]:
                    wait_spread(w, d, e, m)
            for m in held:
                dst = place(w, level(d) * F + flipped(i, m), (e, nb))
                src = piece(w, o, (e, nb)) if m == 0 and d == 0 else dst
                at = ((w * G + d) * nb + e) * F + m + bits[stage]
                flights.send(src, dst, wp_send.at[at], wp_recv.at[at], (o * F + flipped(i, bits[stage]), t))

    def wait_last(w, d):
        for e in range(nb):
            for m in range(1, F):
                if m & order(e)[nb - 1]:
                    wait_spread(w, d, e, m)

    def wait_weights(w):
        local[1 + w].wait()
        for d in range(G):
            wait_last(w, d)

    phase("first_sends")
    swap(0)
    for w in range(2):
        spread(w, 0, 0)
    tot_in[o] = jnp.zeros(tot_in.shape[1:], BF)

    phase("setup")
    for copy in staged[: len(early)]:
        copy.wait()
    row = lax.broadcasted_iota(jnp.int32, (length, length), 0)
    column = lax.broadcasted_iota(jnp.int32, (length, length), 1)
    identity = jnp.where(row == column, 1.0, 0.0).astype(F32)
    R = 2 * heads
    which = lax.broadcasted_iota(jnp.int32, (R, length), 0)
    lane = lax.broadcasted_iota(jnp.int32, (R, length), 1)
    speed = jnp.zeros((R, length), F32)
    for g in range(2):
        for h in range(heads):
            speed = jnp.where(which == g * heads + h, speed_ref[g, h], speed)

    def both(ref):
        return jnp.concatenate([ref[0], ref[1]], axis=0)

    raw = both(shrink_ref)
    softplus = jnp.maximum(raw, 0.0) + jnp.log(1.0 + jnp.exp(-jnp.abs(raw)))
    total_c = both(spike_ref) - speed * softplus
    step = 1
    while step < length:
        ahead = jnp.where(lane >= step, pltpu.roll(total_c, step, 1), 0.0)
        behind = jnp.where(lane < length - step, pltpu.roll(total_c, length - step, 1), 0.0)
        total_c = total_c + jnp.where(which < heads, ahead, behind)
        step = step * 2
    cum = total_c
    total = jnp.where(which[:, :1] < heads, cum[:, length - 1 :], cum[:, :1])
    beta = 1.0 / (1.0 + jnp.exp(-both(insert_ref)))
    pad = jnp.zeros((length - 2 * R, length), F32)
    turned = jnp.transpose(jnp.concatenate([cum, beta, pad], axis=0))

    inside = (column <= row, column >= row)
    proper = (column < row, column > row)

    def crossing(b, g):
        near = row // (2 * b) == column // (2 * b)
        low = ((row // b) % 2 == 1) & ((column // b) % 2 == 0)
        high = ((row // b) % 2 == 0) & ((column // b) % 2 == 1)
        return near & (low if g == 0 else high)

    batch = min(heads, 2)
    for first in range(0, heads, batch):
        phase("local_attention")
        some = range(first, first + batch)
        problems = [(h, g) for h in some for g in range(2)]
        keys, queries, keys_b, like, asked = {}, {}, {}, {}, {}
        for h in some:
            k = k_ref[:, h * DK : (h + 1) * DK].astype(F32)
            q = q_ref[:, h * DK : (h + 1) * DK].astype(F32)
            keys[h] = k * lax.rsqrt(jnp.sum(k * k, axis=-1, keepdims=True) + EPS)
            queries[h] = q * (lax.rsqrt(jnp.sum(q * q, axis=-1, keepdims=True) + EPS) * DK ** (-0.5))
            keys_b[h] = keys[h].astype(BF)
            like[h] = dot_last(keys_b[h], keys_b[h])
            asked[h] = dot_last(queries[h].astype(BF), keys_b[h])
        cum_col, beta_col, decay, strict, inverse = {}, {}, {}, {}, {}
        for p in problems:
            h, g = p
            r = g * heads + h
            cum_col[p] = turned[:, r : r + 1]
            beta_col[p] = turned[:, R + r : R + r + 1]
            gap = jnp.where(inside[g], cum_col[p] - cum[r : r + 1, :], -1e30)
            decay[p] = jnp.exp(gap)
            strict[p] = jnp.where(proper[g], like[h] * decay[p] * beta_col[p], 0.0)
            inverse[p] = identity - jnp.where(crossing(1, g), strict[p], 0.0)
        b = 2
        while b < length:
            half, part = {}, {}
            for p in problems:
                half[p] = inverse[p].astype(BF)
                part[p] = jnp.where(crossing(b, p[1]), strict[p], 0.0).astype(BF)
            for p in problems:
                part[p] = dot(part[p], half[p]).astype(BF)
            for p in problems:
                inverse[p] = inverse[p] - dot(half[p], part[p])
            b = b * 2
        solved = {}
        for p in problems:
            h, g = p
            v = v_ref[:, h * DV : (h + 1) * DV].astype(F32)
            lift = jnp.exp(cum_col[p])
            right = jnp.concatenate(
                [(v * beta_col[p]).astype(BF), (keys[h] * (beta_col[p] * lift)).astype(BF)], axis=-1
            )
            solved[p] = dot(inverse[p].astype(BF), right).astype(BF)
        for p in problems:
            h, g = p
            r = g * heads + h
            lift = jnp.exp(cum_col[p])
            seen = dot((asked[h] * decay[p]).astype(BF), solved[p])
            reach[h, :, g * DK : (g + 1) * DK] = (queries[h] * lift - seen[:, DV:]).astype(BF)
            if g == 0:
                start[h] = seen[:, :DV]
            else:
                start[h] = start[h] + seen[:, :DV]
            fading = keys[h] * jnp.exp(total[r : r + 1, :] - cum_col[p])
            kept = dot_first(solved[p], fading.astype(BF))
            maps_out[h, g, :DK] = (identity * (jnp.exp(total[r : r + 1, :]) - 1.0) - kept[DV:]).astype(BF)
            maps_out[h, g, DK:] = kept[:DV].astype(BF)
        phase("send_maps")
        for h in some:
            flights.send(
                maps_out.at[h], maps_in.at[i], map_send.at[h], map_recv.at[i], (o * F + h, t), when=i != h
            )

            @pl.when(i == h)
            def _():
                maps_in[h] = maps_out[h]

    phase("spread_own")
    for w in range(2):
        spread(w, 0, 1)
    spread(2, 0, 0)

    phase("wait_maps")
    for j in range(F):

        @pl.when(i != j)
        def _():
            landed(maps_in.at[j], map_send.at[j], map_recv.at[j], (s, other))

    phase("compose")
    def turn(g, j):
        return j if g == 0 else F - 1 - j

    whole_maps = []
    for g in range(2):
        whole_maps.append(maps_in[turn(g, 0), g].astype(F32))
    for j in range(1, F):
        for g in range(2):
            at = turn(g, j)
            whole_maps[g] = carry_on(whole_maps[g], maps_in[at, g, :DK]) + maps_in[at, g].astype(F32)
    for g in range(2):
        tot_out[g] = whole_maps[g].astype(BF)
    phase("send_totals")
    for r in range(1, G):
        flights.send(
            tot_out.at[(o // (1 << (r.bit_length() - 1))) % 2], tot_in.at[o], tot_send.at[r], tot_recv.at[r], (level(r) * F + i, t)
        )
    phase("spread_0_0")
    for d in range(1, G):
        spread(0, d, 0)
    phase("wait_totals")
    for r in range(1, G):
        landed(tot_in.at[level(r)], tot_send.at[r], tot_recv.at[r], (s, other))
    swap(1)
    phase("states")
    states = [jnp.zeros((DV, DK), F32) for _ in range(2)]
    for j in range(G - 1):
        for g in range(2):
            at = j if g == 0 else G - 1 - j
            counts = (at < o) if g == 0 else (at > o)
            m = jnp.where(counts, tot_in[at].astype(F32), 0.0)
            states[g] = carry_on(states[g], m[:DK].astype(BF)) + m[DK:]
    for j in range(F):
        for g in range(2):
            at = turn(g, j)
            st_out[at, :, g * DK : (g + 1) * DK] = states[g].astype(BF)
            if j < F - 1:
                states[g] = carry_on(states[g], maps_in[at, g, :DK]) + maps_in[at, g, DK:].astype(F32)
    phase("send_states")
    for r in range(1, F):
        to = (i + r) % F
        flights.send(st_out.at[to], st_in.at[i], st_send.at[r], st_recv.at[r], (o * F + to, t))
    st_in[i] = st_out[i]
    spread(2, 0, 1)
    phase("wait_states")
    for r in range(1, F):
        landed(st_in.at[(i + F - r) % F], st_send.at[r], st_recv.at[r], (s, other))

    phase("outputs")
    for copy in staged[len(early) :]:
        copy.wait()
    for h in range(heads):
        mixture = start[h] + dot_last(reach[h], st_in[h])
        scale = lax.rsqrt(jnp.mean(mixture * mixture, axis=-1, keepdims=True) + EPS)
        valve = z_ref[:, h * DV : (h + 1) * DV].astype(F32)
        gated = mixture * scale * head_gain_ref[...] * silu(valve)
        mixbuf[t, :, h * DV : (h + 1) * DV] = gated.astype(BF)
    flights.send(mixbuf.at[t], mixbuf.at[t], mix_send, mix_recv, (s, other))
    phase("spread_0_1")
    for d in range(1, G):
        spread(0, d, 1)
    phase("project")
    local[0].wait()
    wide = heads * DV
    projected = dot(mixbuf[t], fm[pl.ds(pl.multiple_of(t * wide, 128), wide), :])
    phase("wait_mix")
    landed(mixbuf.at[other], mix_send, mix_recv, (s, other))
    phase("middle")
    projected = projected + dot(mixbuf[other], fm[pl.ds(pl.multiple_of(other * wide, 128), wide), :])
    middle = (skip_ref[...].astype(F32) + projected).astype(BF)
    tok[o, t] = middle

    def share(block, when=True):
        flights.send(
            tok.at[block, t], tok.at[block, t], half_send.at[block], half_recv.at[block], (s, other), when=when
        )

    def pass_up(block, when):
        flights.send(
            tok.at[block, t], tok.at[block, t], tok_send.at[block], tok_recv.at[block],
            (s + F, t), when=when & (o < G - 1),
        )

    def pass_down(block, when):
        flights.send(
            tok.at[block, t], tok.at[block, t], tok_send.at[G + block], tok_recv.at[block],
            (s - F, t), when=when & (o > 0),
        )

    def share_halo(r):
        phase("relay_halo")
        block = flipped(o, r)
        landed(halo.at[block, t], halo_send.at[r], halo_recv.at[block], (s, other))
        flights.send(
            halo.at[block, t], halo.at[block, t], hh_send.at[block], hh_recv.at[block], (s, other)
        )

    def arrive(distance):
        for below in (True, False):
            block = o - distance if below else o + distance
            there = block >= 0 if below else block < G

            @pl.when(there)
            def _():
                landed(tok.at[block, t], tok_send.at[block], tok_recv.at[block], (s, other))

            share(block, when=there)
            (pass_up if below else pass_down)(block, there)

    pass_up(o, o >= 0)
    pass_down(o, o >= 0)
    share(o)
    strips = feats // 128
    ends = jnp.concatenate([middle[:1], middle[length - 1 :]], axis=0).astype(F32)
    edge_out[...] = jnp.concatenate(
        [ends[e : e + 1, c * 128 : (c + 1) * 128] for e in range(2) for c in range(strips)], axis=0
    ).astype(BF)
    flights.send(edge_out, edge_in.at[0], edge_send.at[0], edge_recv.at[0], (after, t))
    flights.send(edge_out, edge_in.at[1], edge_send.at[1], edge_recv.at[1], (before, t))
    def normed(rows0, rows1):
        squares = jnp.sum(rows0 * rows0, axis=-1, keepdims=True) + jnp.sum(rows1 * rows1, axis=-1, keepdims=True)
        scale = lax.rsqrt(squares * (1.0 / (2 * feats)) + EPS)
        return (
            (rows0 * scale * row_gain_ref[:, :feats]).astype(BF),
            (rows1 * scale * row_gain_ref[:, feats:]).astype(BF),
        )

    def strip_rows(block, half):
        rows = []
        for side in range(2):
            packed = halo[block, half, side].astype(F32)
            base = (1 - side) * strips
            rows.append(jnp.concatenate([packed[base + c : base + c + 1] for c in range(strips)], axis=1))
        return jnp.concatenate(rows + [jnp.zeros((14, feats), F32)], axis=0)

    my_taps = taps_ref[:, pl.ds(pl.multiple_of(o * units, 128), units)]
    row_u = lax.broadcasted_iota(jnp.int32, (length, units), 0)

    def work(r):
        block = flipped(o, r)
        phase("wait_rows_from_core")
        landed(tok.at[block, other], half_send.at[block], half_recv.at[block], (s, other))
        landed(halo.at[block, other], hh_send.at[block], hh_recv.at[block], (s, other))
        phase("ffn_in")
        a, b2 = normed(tok[block, 0].astype(F32), tok[block, 1].astype(F32))
        nrm[:length, :feats] = a
        nrm[:length, feats:] = b2
        a, b2 = normed(strip_rows(block, 0), strip_rows(block, 1))
        nrm[length:, :feats] = a
        nrm[length:, feats:] = b2
        gate = dot(nrm[...], wv[...].reshape(2 * feats, units)).astype(BF).astype(F32)
        up = dot(nrm[:length], wu[...].reshape(2 * feats, units))
        at = block * F + i
        first_row = jnp.where(at > 0, gate[length : length + 1], 0.0)
        last_row = jnp.where(at < n - 1, gate[length + 1 : length + 2], 0.0)
        here = gate[:length]
        earlier = jnp.where(row_u == 0, first_row, pltpu.roll(here, 1, 0))
        later = jnp.where(row_u == length - 1, last_row, pltpu.roll(here, length - 1, 0))
        convolved = earlier * my_taps[0:1] + here * my_taps[1:2] + later * my_taps[2:3]
        hid[r] = (silu(convolved) * up).astype(BF)

    parts = G // 2
    chunk = F * cols

    def down(d, some):
        first, size = some
        lev = level(d)
        home, q = lev // parts, lev % parts
        rows = pl.ds(first, size)
        product = dot(
            hid[rows].reshape(size * length, units), wn[:, pl.ds(pl.multiple_of(lev * chunk, 128), chunk)]
        )

        @pl.when(home != t)
        def _():
            x_out[q, rows] = product.astype(BF).reshape(size, length, chunk)

        flights.send(
            x_out.at[q, rows], x_in.at[q, rows], x_send.at[q * G + first], x_recv.at[q * G + first],
            (s, other), when=home != t,
        )

        @pl.when(home == t)
        def _():
            mine[q, rows] = product.astype(BF).reshape(size, length, chunk)

    def settle(d, some):
        first, size = some
        lev = level(d)
        home, q = lev // parts, lev % parts
        rows = pl.ds(first, size)

        @pl.when(home == t)
        def _():
            landed(x_in.at[q, rows], x_send.at[q * G + first], x_recv.at[q * G + first], (s, other))
            z_out[q, rows] = (mine[q, rows].astype(F32) + x_in[q, rows].astype(F32)).astype(BF)

        for r in range(max(first, 1), first + size):
            flights.send(
                z_out.at[q, r], z_in.at[o, q], z_send.at[q * G + r], z_recv.at[o * parts + q],
                (level(r) * F + i, t), when=home == t,
            )

    swap(2, [1])
    phase("spread_1_0")
    for d in range(1, G):
        spread(1, d, 0)
    phase("rows_1")
    arrive(1)
    phase("spread_1_1")
    for d in range(1, G):
        spread(1, d, 1)
    phase("wait_edges")
    landed(edge_in.at[0], edge_send.at[0], edge_recv.at[0], (s, other))
    landed(edge_in.at[1], edge_send.at[1], edge_recv.at[1], (s, other))
    halo[o, t] = edge_in[...]
    for r in range(1, G):
        flights.send(edge_in, halo.at[o, t], halo_send.at[r], halo_recv.at[o], (level(r) * F + i, t))
    flights.send(edge_in, halo.at[o, t], hh_send.at[o], hh_recv.at[o], (s, other))
    swap(2, range(2, G))
    phase("spread_2_0")
    spread(2, 1, 0)
    for distance in range(2, G - 1):
        phase("rows_2")
        arrive(distance)
    for r in range(1, G):
        share_halo(r)
    phase("wait_weights")
    wait_weights(0)
    wait_weights(1)
    near, far, every = (0, G // 2), (G // 2, G // 2), (0, G)
    for r in range(G // 2):
        work(r)
    phase("rows_3")
    arrive(G - 1)
    phase("spread_2_0")
    for d in range(2, G):
        spread(2, d, 0)
    spread(2, 1, 1)
    phase("down_own")
    wait_last(2, 0)
    local[3].wait()
    down(0, near)
    phase("settle_own")
    settle(0, near)
    for r in range(G // 2, G):
        work(r)
    phase("down_own")
    down(0, far)
    phase("spread_2_1")
    for d in range(2, G):
        spread(2, d, 1)
    settle(0, far)
    for d in range(1, G):
        phase("wait_narrowing")
        wait_last(2, d)
        phase("down")
        down(d, every)
        phase("settle")
        settle(d, every)
    phase("result")
    for q in range(parts):
        at = slice(q * chunk, (q + 1) * chunk)
        result = tok[o, t, :, at].astype(F32) + z_out[q, 0].astype(F32)
        for r in range(1, G):
            lev = level(r)
            landed(z_in.at[lev, q], z_send.at[q], z_recv.at[lev * parts + q], (s, other))
            result = result + z_in[lev, q].astype(F32)
        out_ref[:, at] = result.astype(BF)

    phase("finish")
    flights.finish()

    phase(None)


def fits(n, tp, length, feats, heads, units, rows, cols):
    group = group_size(n)
    far = n // group
    return (
        tp == 2 and group > 1 and far == heads and far & (far - 1) == 0 and heads % 2 == 0
        and length == DK and DK == DV and feats % 128 == 0
        and units % group == 0 and (units // group) % 128 == 0 and cols % 128 == 0 and rows % 16 == 0
    )


def fused_body(
    skip_pathway, request_vectors, lookup_address_matrix, content_vectors, result_valve_matrix,
    shrink_raw_signal, channel_shrink_speed, insertion_raw_signal, extra_shrink_spike,
    channel_scaling_vector, final_mapping_matrix, mixer_scaling_vector, valve_matrix,
    widening_matrix, temporal_kernel_entries, narrowing_matrix,
):
    n = lax.axis_size("sp")
    G = group_size(n)
    F = n // G
    length, feats = skip_pathway.shape
    heads = request_vectors.shape[1] // DK
    rows = valve_matrix.shape[0]
    units = valve_matrix.shape[1] // G
    strips = feats // 128
    vmem, anywhere = pl.BlockSpec(memory_space=pltpu.VMEM), pl.BlockSpec(memory_space=pl.ANY)
    dma = pltpu.SemaphoreType.DMA
    head_gain = channel_scaling_vector.reshape(1, -1)
    row_gain = mixer_scaling_vector.reshape(1, -1)
    staged = [
        skip_pathway, request_vectors, lookup_address_matrix, content_vectors, result_valve_matrix,
        shrink_raw_signal, channel_shrink_speed, insertion_raw_signal, extra_shrink_spike,
        head_gain, row_gain, temporal_kernel_entries,
    ]
    stages = [
        pltpu.SMEM(x.shape, x.dtype) if x is channel_shrink_speed else pltpu.VMEM(x.shape, x.dtype)
        for x in staged
    ]
    return pl.pallas_call(
        functools.partial(layer_kernel, n, G),
        out_shape=jax.ShapeDtypeStruct((length, feats), BF),
        in_specs=[anywhere] * 16,
        out_specs=vmem,
        scratch_shapes=stages + [
            dma((len(staged),)),
            pltpu.VMEM(final_mapping_matrix.shape, BF),
            pltpu.VMEM((n, rows, units), BF),
            pltpu.VMEM((n, rows, units), BF),
            pltpu.VMEM((units, 2 * feats), BF),
            pltpu.VMEM((heads, 2, DK + DV, DK), BF),
            pltpu.VMEM((F, 2, DK + DV, DK), BF),
            pltpu.VMEM((2, DK + DV, DK), BF),
            pltpu.VMEM((G, DK + DV, DK), BF),
            pltpu.VMEM((F, DV, 2 * DK), BF),
            pltpu.VMEM((heads, DV, 2 * DK), BF),
            pltpu.VMEM((heads, length, 2 * DK), BF),
            pltpu.VMEM((heads, length, DV), F32),
            pltpu.VMEM((2, length, heads * DV), BF),
            pltpu.VMEM((G, 2, length, feats), BF),
            pltpu.VMEM((length + 16, 2 * feats), BF),
            pltpu.VMEM((2 * strips, 128), BF),
            pltpu.VMEM((2, 2 * strips, 128), BF),
            pltpu.VMEM((G, 2, 2, 2 * strips, 128), BF),
            pltpu.VMEM((G, length, units), BF),
            pltpu.VMEM((G // 2, G, length, 2 * feats // G), BF),
            pltpu.VMEM((G // 2, G, length, 2 * feats // G), BF),
            pltpu.VMEM((G // 2, G, length, 2 * feats // G), BF),
            pltpu.VMEM((G // 2, G, length, 2 * feats // G), BF),
            pltpu.VMEM((G, G // 2, length, 2 * feats // G), BF),
            dma((4,)),
            dma((3 * G,)), dma((3 * G,)),
            dma((3 * G * F * (F.bit_length() - 1),)), dma((3 * G * F * (F.bit_length() - 1),)),
            dma((F,)), dma((F,)),
            dma((G,)), dma((G,)),
            dma((F,)), dma((F,)),
            dma, dma,
            dma((2,)), dma((2,)),
            dma((2 * G,)), dma((G,)),
            dma((G,)), dma((G,)),
            dma((G,)), dma((G,)),
            dma((G,)), dma((G,)),
            dma((G * G // 2,)), dma((G * G // 2,)),
            dma((G * G // 2,)), dma((G * G // 2,)),
        ],
        compiler_params=pltpu.CompilerParams(
            collective_id=0, has_side_effects=True, vmem_limit_bytes=60 * 1024 * 1024
        ),
        name="layer",
    )(
        skip_pathway, request_vectors, lookup_address_matrix, content_vectors, result_valve_matrix,
        shrink_raw_signal, channel_shrink_speed, insertion_raw_signal, extra_shrink_spike,
        head_gain, final_mapping_matrix, row_gain,
        valve_matrix, widening_matrix, temporal_kernel_entries, narrowing_matrix,
    )


def body(*arrays):
    skip, queries = arrays[0], arrays[1]
    valve, narrowing = arrays[12], arrays[15]
    n, tp = lax.axis_size("sp"), lax.axis_size("tp")
    if fits(n, tp, *skip.shape, queries.shape[1] // DK, valve.shape[1], valve.shape[0], narrowing.shape[1]):
        return fused_body(*arrays)
    return plain_body(*arrays)


def solution(mesh):
    return jax.shard_map(
        body,
        mesh=mesh,
        in_specs=(
            P("sp", "tp"),
            P("sp", "tp"),
            P("sp", "tp"),
            P("sp", "tp"),
            P("sp", "tp"),
            P(None, "tp", "sp"),
            P(None, "tp"),
            P(None, "tp", "sp"),
            P(None, "tp", "sp"),
            P(),
            P(None, "tp"),
            P(),
            P("sp", "tp"),
            P("sp", "tp"),
            P(None, "tp"),
            P("tp", "sp"),
        ),
        out_specs=P("sp", "tp"),
        check_vma=False,
    )
```
